128 devices in a mesh: sp: 16 (over z, y), dp: 8 (over x, core).
Axes of the slice: x: 4, y: 4, z: 4, core: 2. Of those that a mesh axis runs over, the one named last changes fastest.
Arguments:
- tokens: bfloat16 [8, 5120, 2048], P('dp', 'sp'), may hold values from -6 to 6
- w_query: bfloat16 [2048, 1024], P('dp', 'sp'), may hold values from -0.125 to 0.125
- w_key: bfloat16 [2048, 1024], P('dp', 'sp'), may hold values from -0.125 to 0.125
- w_value: bfloat16 [2048, 1024], P('dp', 'sp'), may hold values from -0.125 to 0.125
- w_output: bfloat16 [1024, 2048], P('sp', 'dp'), may hold values from -0.1875 to 0.1875
- qk_gain: float32 [2, 64], replicated, may hold values from 0.4 to 7
- decay_sums: float32 [8, 16, 5120], P('dp', 'sp'), may hold values from -1024 to 0, as said below
Outputs:
- layer_out: bfloat16 [8, 5120, 2048], P('dp', 'sp')
The draws below stay inside these ranges and needn't reach their ends.
Inputs may be any that keep to these rules, and one draw needn't show every extreme that they name: `decay_sums`: each row is non-increasing along positions.
All inputs are finite; a program needn't handle non-finite values.
Results may differ from the reference program's by a relative error of at most 0.0075.
The reference program's roundings to bfloat16 on the way (of `query_proj`, `key_proj`, `value_proj`, `query_unit`, `key_unit`, `probs` and `head_out`) count: a program that leaves them out, or rounds other values in their place, can miss the bound.
Values may be sent and summed in bfloat16 or wider, within the bound.
No kernel may reach another device: no remote copies, remote signals or barrier semaphores. Data moves between devices by JAX's collectives and lax.ppermute only.
A program may use at most 128 MiB of HBM per device.

```python
import jax
import jax.numpy as jnp
from jax import lax

D = 2048
HEADS = 16
HEAD_DIM = 64
TOK_DEV = 320
LENGTH = 5120
SEQS = 8


def draw_qk_gain(key, part):
    return jnp.clip(1.0 + 0.25 * jax.random.normal(key, (2, HEAD_DIM), jnp.float32), 0.4, 1.8)


def draw_decay_sums(key, part):
    streams = jax.random.split(key, 5)
    chance = 0.5
    quick = jax.random.bernoulli(streams[0], chance, (SEQS, HEADS, 1))
    quick_rate = 1.0 / jax.random.uniform(streams[1], (SEQS, HEADS, 1), jnp.float32, 30.0, 100.0)
    slow_rate = jax.random.uniform(streams[2], (SEQS, HEADS, 1), jnp.float32, 0.2, 0.8) / LENGTH
    rate = jnp.where(quick, quick_rate, slow_rate)
    spans = LENGTH // TOK_DEV
    factor = jnp.exp(jax.random.uniform(streams[3], (SEQS, HEADS, spans), jnp.float32, -1.05, 1.05))
    factor = jnp.repeat(factor, TOK_DEV, axis=2)
    rough = jax.random.uniform(streams[4], (SEQS, HEADS, LENGTH), jnp.float32, 0.2, 1.8)
    return -jnp.cumsum(rate * factor * rough, axis=2)


def steps_of(own_key, dims, shards, smallest, largest):
    level, own = 1.0, jax.random.fold_in(own_key, 6)
    for position, parts in shards:
        heights = jnp.exp(jax.random.uniform(jax.random.fold_in(own, position), (parts,), jnp.float32, smallest / len(shards), largest / len(shards)))
        level = level * jnp.repeat(heights, dims[position] // parts).reshape([-1 if axis == position else 1 for axis in range(len(dims))])
    return level


def normal_values(rng, extent, width, bound, pieces=(), held_as=jnp.bfloat16):
    level = steps_of(rng, extent, pieces, -0.22, 0.18) if pieces else 1.0
    drawn = jax.random.normal(rng, extent, jnp.float32) * width * level
    return jnp.minimum(jnp.maximum(drawn, -bound), bound).astype(held_as)


def setup_inputs(seed: int = 0) -> dict:
    key_of = jax.random.split(jax.random.key(seed), 8)
    return {
        "tokens": normal_values(key_of[0], (SEQS, LENGTH, D), 1.0, 6.0, ((0, 8), (1, 16))),
        "w_query": normal_values(key_of[1], (D, HEADS * HEAD_DIM), D ** -0.5, 0.125, ((0, 8), (1, 16))),
        "w_key": normal_values(key_of[2], (D, HEADS * HEAD_DIM), D ** -0.5, 0.125, ((0, 8), (1, 16))),
        "w_value": normal_values(key_of[3], (D, HEADS * HEAD_DIM), D ** -0.5, 0.125, ((0, 8), (1, 16))),
        "w_output": normal_values(key_of[4], (HEADS * HEAD_DIM, D), (HEADS * HEAD_DIM) ** -0.5, 0.1875, ((0, 16), (1, 8))),
        "qk_gain": draw_qk_gain(jax.random.fold_in(key_of[7], 71), 0),
        "decay_sums": draw_decay_sums(jax.random.fold_in(key_of[7], 71), 0),
    }


def normalize(values):
    values = values.astype(jnp.float32)
    return values * lax.rsqrt(lax.optimization_barrier(jnp.mean(values * values, axis=-1, keepdims=True)) + 1e-06)

def attend(query_unit, key_unit, value_rows, decay_rows):
    length = query_unit.shape[0]
    block = min(512, length)
    key_place = jnp.arange(length, dtype=jnp.int32)
    keys_wide = key_unit.astype(jnp.float32)
    values_wide = value_rows.astype(jnp.float32)

    def one_block(index):
        start = (index * block).astype(jnp.int32)
        query_block = lax.dynamic_slice_in_dim(query_unit, start, block, 0).astype(jnp.float32)
        decay_block = lax.dynamic_slice_in_dim(decay_rows, start, block, 1)
        scores = jnp.einsum('qhd,khd->hqk', query_block, keys_wide, precision=lax.Precision.HIGHEST)
        scores = scores + decay_block[:, :, None] - decay_rows[:, None, :]
        query_place = start + jnp.arange(block, dtype=jnp.int32)
        scores = jnp.where(key_place[None, None, :] <= query_place[None, :, None], scores, -jnp.inf)
        peak = lax.optimization_barrier(jnp.max(scores, axis=-1, keepdims=True))
        weights = jnp.exp(scores - peak)
        probs = (weights / lax.optimization_barrier(jnp.sum(weights, axis=-1, keepdims=True))).astype(jnp.bfloat16)
        return jnp.einsum('hqk,khd->qhd', probs.astype(jnp.float32), values_wide, precision=lax.Precision.HIGHEST)
    blocks = lax.map(one_block, jnp.arange(length // block, dtype=jnp.int32))
    return blocks.reshape(length, query_unit.shape[1], query_unit.shape[2])

def reference(tokens, w_query, w_key, w_value, w_output, qk_gain, decay_sums):

    def one_sequence(pair):
        own_rows, decay_rows = pair
        length = own_rows.shape[0]
        query_proj = jnp.dot(own_rows, w_query, preferred_element_type=jnp.float32).astype(jnp.bfloat16)
        key_proj = jnp.dot(own_rows, w_key, preferred_element_type=jnp.float32).astype(jnp.bfloat16)
        value_proj = jnp.dot(own_rows, w_value, preferred_element_type=jnp.float32).astype(jnp.bfloat16)
        query_proj = query_proj.reshape(length, HEADS, HEAD_DIM)
        key_proj = key_proj.reshape(length, HEADS, HEAD_DIM)
        value_proj = value_proj.reshape(length, HEADS, HEAD_DIM)
        query_unit = (normalize(query_proj) * qk_gain[0].astype(jnp.float32) * HEAD_DIM ** (-0.5)).astype(jnp.bfloat16)
        key_unit = (normalize(key_proj) * qk_gain[1].astype(jnp.float32)).astype(jnp.bfloat16)
        attended = attend(query_unit, key_unit, value_proj, decay_rows)
        head_out = normalize(attended).astype(jnp.bfloat16).reshape(length, HEADS * HEAD_DIM)
        return jnp.dot(head_out, w_output, preferred_element_type=jnp.float32).astype(jnp.bfloat16)
    return lax.map(one_sequence, (tokens, decay_sums))
```

```python
import functools

import jax
import jax.numpy as jnp
from jax import lax
from jax.experimental import pallas as pl
from jax.experimental.pallas import tpu as pltpu
from jax.sharding import Mesh
from jax.sharding import PartitionSpec as P


DP = ("dp_0", "dp_1")
SP = ("sp_0", "sp_1")
Z, Y, X, C = "sp_0", "sp_1", "dp_0", "dp_1"
LOG2E = 1.4426950408889634
T = 5120
BLK = 320
BQ = 256
NT = (((1,), (1,)), ((), ()))
NN = (((1,), (0,)), ((), ()))
f32 = jnp.float32
bf16 = jnp.bfloat16


def attn_kernel(pos_ref, fast_ref, kd_ref, qd_ref, *refs, nblk):
    nin=len(nblk)
    ins=refs[:nin]; out_ref=refs[nin]; ka,qa,vs,vt,ot,sbuf=refs[nin+1:]
    lane=lax.broadcasted_iota(jnp.int32,(BLK,128),1)
    lo=lane<64
    lanev=lax.broadcasted_iota(jnp.int32,(BLK//2,128),1)
    tail=jnp.where(lanev==64,1.0,0.0)
    n=0
    for a,nb in zip(ins,nblk):
        for b in range(nb):
            base=pl.multiple_of(pos_ref[n]*BLK,64); n+=1
            qk=a[b*480:b*480+320,:].astype(f32)
            rolled=pltpu.roll(qk,64,1)
            ka[pl.ds(base,BLK),0:128]=jnp.where(lo,rolled,qk).astype(bf16)
            qs=jnp.where(lo,qk,rolled)*LOG2E
            hi=qs.astype(bf16).astype(f32)
            qa[pl.ds(base,BLK),0:128]=jnp.where(lo,hi,qs-hi).astype(bf16)
            v=a[b*480+320:b*480+480,:].astype(f32)
            vs[pl.ds(base,BLK//2),:]=jnp.where(lanev<64,v,tail)
            vs[pl.ds(base+BLK//2,BLK//2),:]=jnp.where(lanev<64,pltpu.roll(v,64,1),tail)
    for i in range(T//512):
        s=slice(i*512,(i+1)*512)
        ka[s,128:256]=kd_ref[s,:]
        qa[s,128:256]=qd_ref[s,:]
    for i in range(T//256):
        vt[:,i*256:(i+1)*256]=vs[i*256:(i+1)*256,:].T[0:80].astype(bf16)

    def finish(acc):
        o=acc[0:64]/acc[64:65]
        return o*lax.rsqrt(jnp.mean(o*o,axis=0,keepdims=True)+1e-6)

    def fast():
        kio=lax.broadcasted_iota(jnp.int32,(BQ,BQ),0); qio=lax.broadcasted_iota(jnp.int32,(BQ,BQ),1)
        keep=kio<=qio
        def per_q(qi,_):
            q0=pl.multiple_of(qi*BQ,BQ)
            qb=qa[pl.ds(q0,BQ),:]
            s=lax.dot_general(ka[pl.ds(q0,BQ),:],qb,NT,preferred_element_type=f32)
            p=jnp.where(keep,jnp.exp2(s),0.0).astype(bf16)
            acc=lax.dot_general(vt[:,pl.ds(q0,BQ)],p,NN,preferred_element_type=f32)
            def chunk(w):
                def body(j,acc):
                    k0=pl.multiple_of(j*w,w)
                    s=lax.dot_general(ka[pl.ds(k0,w),:],qb,NT,preferred_element_type=f32)
                    p=jnp.exp2(s).astype(bf16)
                    return acc+lax.dot_general(vt[:,pl.ds(k0,w)],p,NN,preferred_element_type=f32)
                return body
            W=1024
            nfull=qi*BQ//W
            acc=lax.fori_loop(0,nfull,chunk(W),acc)
            acc=lax.fori_loop(nfull*(W//BQ),qi,chunk(BQ),acc)
            ot[:,pl.ds(q0,BQ)]=finish(acc)
            return 0
        lax.fori_loop(0,T//BQ,per_q,0)

    def slow():
        kio=lax.broadcasted_iota(jnp.int32,(BQ,BQ),0); qio=lax.broadcasted_iota(jnp.int32,(BQ,BQ),1)
        def per_q(qi,_):
            q0=pl.multiple_of(qi*BQ,BQ)
            qb=qa[pl.ds(q0,BQ),:]
            def body(j,c):
                m,acc=c
                k0=pl.multiple_of(j*BQ,BQ)
                s=lax.dot_general(ka[pl.ds(k0,BQ),:],qb,NT,preferred_element_type=f32)
                s=jnp.where(kio+k0<=qio+q0,s,-jnp.inf)
                m2=jnp.maximum(m,jnp.max(s,axis=0,keepdims=True))
                p=jnp.exp2(s-m2).astype(bf16)
                acc=acc*jnp.exp2(m-m2)+lax.dot_general(vt[:,pl.ds(k0,BQ)],p,NN,preferred_element_type=f32)
                return m2,acc
            m0=jnp.full((1,BQ),-jnp.inf,f32)
            c=body(qi,(m0,jnp.zeros((80,BQ),f32)))
            m,acc=lax.fori_loop(0,qi,body,c)
            ot[:,pl.ds(q0,BQ)]=finish(acc)
            return 0
        lax.fori_loop(0,T//BQ,per_q,0)
    isfast=fast_ref[0]>0
    pl.when(isfast)(fast)
    pl.when(jnp.logical_not(isfast))(slow)
    for i in range(T//256):
        s=slice(i*256,(i+1)*256)
        vs[s,0:64]=ot[:,s].T
    for j in range(T//BLK):
        a=vs[j*BLK:j*BLK+160,:]; b=vs[j*BLK+160:(j+1)*BLK,:]
        out_ref[j]=jnp.where(lanev<64,a,pltpu.roll(b,64,1)).astype(bf16)

def decay_cols(d):
    x=d*LOG2E
    h=lax.reduce_precision(x,8,7); r=x-h
    m=lax.reduce_precision(r,8,7); l=lax.reduce_precision(r-m,8,7)
    lane=lax.broadcasted_iota(jnp.int32,(T,128),1)
    c=lambda v: v[:,None]
    kd=jnp.where(lane==0,-c(h),jnp.where(lane==1,-c(m),jnp.where(lane==2,-c(l),jnp.where(lane<6,1.0,0.0))))
    qd=jnp.where(lane==3,c(h),jnp.where(lane==4,c(m),jnp.where(lane==5,c(l),jnp.where(lane<3,1.0,0.0))))
    return kd.astype(bf16),qd.astype(bf16)

def attention(pos,fast,kd,qd,ins,nblk):
    V=pltpu.VMEM
    return pl.pallas_call(functools.partial(attn_kernel,nblk=nblk),
        out_shape=jax.ShapeDtypeStruct((16,160,128),bf16),
        in_specs=[pl.BlockSpec(memory_space=pltpu.SMEM)]*2+[pl.BlockSpec(memory_space=pltpu.VMEM)]*(2+len(ins)),
        out_specs=pl.BlockSpec(memory_space=pltpu.VMEM),
        scratch_shapes=[V((T,256),bf16),V((T,256),bf16),V((T,128),f32),V((80,T),bf16),V((64,T),f32),V((8,128),f32)],
        compiler_params=pltpu.CompilerParams(vmem_limit_bytes=50*1024*1024),
        name="attention")(pos,fast,kd,qd,*ins)


def proj_kernel(idx_ref, gain_ref, *refs, pieces):
    per = [sum(p) for p in pieces]
    ntok = sum(len(p) for p in pieces)
    toks = refs[: ntok * 8]
    ws = refs[ntok * 8 : ntok * 8 + 4]
    out_ref = refs[ntok * 8 + 4]
    lane = lax.broadcasted_iota(jnp.int32, (BLK, 128), 1)
    lo = lane < 64
    half = lax.broadcasted_iota(jnp.int32, (BLK // 2, 128), 1) < 64
    at = 0
    for b, piece in enumerate(pieces):
        acc = [None, None]
        for dx in range(4):
            for c in range(2):
                parts = [toks[(at + n) * 8 + dx * 2 + c][...] for n in range(len(piece))]
                tok = parts[0] if len(parts) == 1 else jnp.concatenate(parts, 0)
                rhs = jnp.concatenate([ws[dx][c * 256 : c * 256 + 256, :], ws[dx][512:768, :]], 1)
                part = lax.dot_general(tok, rhs, NN, preferred_element_type=f32)
                acc[c] = part if acc[c] is None else acc[c] + part
        at += len(piece)
        qk = (acc[0][:, :128] + acc[1][:, :128]).astype(bf16).astype(f32)
        sq = qk * qk
        s_lo = jnp.sum(jnp.where(lo, sq, 0.0), axis=1, keepdims=True)
        s_hi = jnp.sum(jnp.where(lo, 0.0, sq), axis=1, keepdims=True)
        inv = jnp.where(lo, lax.rsqrt(s_lo * (1 / 64) + 1e-6), lax.rsqrt(s_hi * (1 / 64) + 1e-6))
        out_ref[b * 480 : b * 480 + 320, :] = (qk * inv * gain_ref[...]).astype(bf16)
        s, t = acc[0][:, 128:], acc[1][:, 128:]
        top = s[:160] + pltpu.roll(t[:160], 64, 1)
        bot = pltpu.roll(s[160:], 64, 1) + t[160:]
        out_ref[b * 480 + 320 : b * 480 + 480, :] = jnp.where(half, top, bot).astype(bf16)


def project(xidx, gains, pieces, ws):
    sizes = tuple(tuple(p.shape[0] for p in ps) for ps in pieces)
    args, specs = [], []
    for ps in pieces:
        for p in ps:
            for dx in range(4):
                for c in range(2):
                    args.append(p)
                    specs.append(
                        pl.BlockSpec((p.shape[0], 256), lambda i, idx, dx=dx, c=c: (0, 2 * idx[dx] + c))
                    )
    nb = len(pieces)
    return pl.pallas_call(
        functools.partial(proj_kernel, pieces=sizes),
        out_shape=jax.ShapeDtypeStruct((4, nb * 480, 128), bf16),
        grid_spec=pltpu.PrefetchScalarGridSpec(
            num_scalar_prefetch=1,
            grid=(4,),
            in_specs=[pl.BlockSpec((1, 128), lambda i, idx: (0, 0))]
            + specs
            + [pl.BlockSpec((768, 128), lambda i, idx: (i, 0))] * 4,
            out_specs=pl.BlockSpec((None, nb * 480, 128), lambda i, idx: (i, 0, 0)),
        ),
        compiler_params=pltpu.CompilerParams(vmem_limit_bytes=40 * 1024 * 1024),
        name="project",
    )(xidx, gains, *args, *ws)


def out_kernel(heads_ref, w_ref, o_ref, lhs):
    @pl.when(pl.program_id(0) == 0)
    def _():
        half = lax.broadcasted_iota(jnp.int32, (BLK // 2, 128), 1) < 64
        for p in range(8):
            a = heads_ref[2 * p].astype(f32)
            b = heads_ref[2 * p + 1].astype(f32)
            s = slice(p * 128, p * 128 + 128)
            lhs[0:160, s] = jnp.where(half, a, pltpu.roll(b, 64, 1)).astype(bf16)
            lhs[160:320, s] = jnp.where(half, pltpu.roll(a, 64, 1), b).astype(bf16)

    rhs = jnp.concatenate(
        [w_ref[:, 0, 0].reshape(1024, 128), w_ref[:, 0, 1].reshape(1024, 128)], 1
    )
    o_ref[...] = lax.dot_general(lhs[...], rhs, NN, preferred_element_type=f32).astype(bf16)


def output(heads, w_all):
    return pl.pallas_call(
        out_kernel,
        out_shape=jax.ShapeDtypeStruct((BLK, 2048), bf16),
        grid=(8,),
        in_specs=[
            pl.BlockSpec((16, 160, 128), lambda i: (0, 0, 0)),
            pl.BlockSpec((16, 1, 2, 64, 128), lambda i: (0, i, 0, 0, 0)),
        ],
        out_specs=pl.BlockSpec((BLK, 256), lambda i: (0, i)),
        scratch_shapes=[pltpu.VMEM((BLK, 1024), bf16)],
        name="output",
    )(heads, w_all)


def turn(step):
    return [(i, (i + step) % 4) for i in range(4)]


def on_device(tokens, w_query, w_key, w_value, w_output, qk_gain, decay_sums):
    own = tokens[0]
    z, y, x, c = (lax.axis_index(a) for a in (Z, Y, X, C))
    t1 = lax.ppermute(own, Y, turn(-1))
    t3 = lax.ppermute(own, Y, turn(1))
    t2 = [lax.ppermute(t1[:160], Y, turn(-1)), lax.ppermute(t3[160:], Y, turn(1))]
    own_qk = jnp.concatenate([w_query, w_key], 1)
    swap = lax.ppermute(
        jnp.concatenate([own_qk, jnp.pad(w_value, ((0, 0), (0, 64)))], 0), C, [(0, 1), (1, 0)]
    )
    other_qk, other_v = swap[:256], swap[256:, :64]
    first = c == 0
    piece = jnp.concatenate(
        [
            jnp.where(first, own_qk, other_qk),
            jnp.where(first, other_qk, own_qk),
            jnp.concatenate(
                [jnp.where(first, w_value, other_v), jnp.where(first, other_v, w_value)], 1
            ),
        ],
        0,
    )
    w4 = jnp.concatenate([piece] + [lax.ppermute(piece, Z, turn(-d)) for d in (1, 2, 3)], 0)
    ws = [w4] + [lax.ppermute(w4, X, turn(-d)) for d in (1, 2, 3)]
    wo = jnp.concatenate([w_output[:, :128], w_output[:, 128:]], 0)
    wo_all = lax.all_gather(wo, SP + DP, axis=0).reshape(16, 8, 2, 64, 128)

    xidx = jnp.stack([(x + d) % 4 for d in range(4)]).astype(jnp.int32)
    gains = jnp.concatenate([qk_gain[0] * 0.125, qk_gain[1]])[None]
    part1 = project(xidx, gains, [[own], [t1], [t3]], ws)
    part2 = project(xidx, gains, [t2], ws)
    recv = []
    for part in (part1, part2):
        recv += [part[0]] + [lax.ppermute(part[d], Z, turn(d)) for d in (1, 2, 3)]
    pos = [4 * ((z - d) % 4) + (y + e) % 4 for d in range(4) for e in (0, 1, 3)]
    pos += [4 * ((z - d) % 4) + (y + 2) % 4 for d in range(4)]
    pos = jnp.stack(pos).astype(jnp.int32)
    bound = jnp.max(jnp.abs(qk_gain[0])) * jnp.max(jnp.abs(qk_gain[1]))
    fast = (bound <= 7.7).astype(jnp.int32)[None]
    kd, qd = decay_cols(decay_sums[0, 0])
    heads = attention(pos, fast, kd, qd, recv, (3, 3, 3, 3, 1, 1, 1, 1))
    merged = lax.all_to_all(heads, SP, 0, 0, tiled=True)
    return output(merged, wo_all)[None]


def solution(mesh):
    torus = Mesh(mesh.devices.reshape(4, 4, 4, 2), ("sp_0", "sp_1", "dp_0", "dp_1"))
    in_specs = (P(DP, SP, None), P(DP, SP), P(DP, SP), P(DP, SP), P(SP, DP), P(), P(DP, SP, None))
    out_specs = P(DP, SP, None)
    return jax.shard_map(
        on_device, mesh=torus, in_specs=in_specs, out_specs=out_specs, check_vma=False
    )
```

```python
import functools

import jax
import jax.numpy as jnp
from jax import lax
from jax.experimental import pallas as pl
from jax.experimental.pallas import tpu as pltpu
from jax.sharding import Mesh
from jax.sharding import PartitionSpec as P


DP = ("dp_0", "dp_1")
SP = ("sp_0", "sp_1")
Z, Y, X, C = "sp_0", "sp_1", "dp_0", "dp_1"
LOG2E = 1.4426950408889634
T = 5120
BLK = 320
BQ = 512
W = 1024
NT = (((1,), (1,)), ((), ()))
NN = (((1,), (0,)), ((), ()))
f32 = jnp.float32
bf16 = jnp.bfloat16


def attn_kernel(pos_ref, fast_ref, kd_ref, qd_ref, *refs, nblk):
    nin=len(nblk)
    ins=refs[:nin]; out_ref=refs[nin]; ka,qa,vs,vt,ot=refs[nin+1:]
    lane=lax.broadcasted_iota(jnp.int32,(BLK,128),1)
    lo=lane<64
    lanev=lax.broadcasted_iota(jnp.int32,(BLK//2,128),1)
    tail=jnp.where(lanev==64,1.0,0.0)
    n=0
    for a,nb in zip(ins,nblk):
        for b in range(nb):
            base=pl.multiple_of(pos_ref[n]*BLK,64); n+=1
            qk=a[b*480:b*480+320,:].astype(f32)
            rolled=pltpu.roll(qk,64,1)
            ka[pl.ds(base,BLK),0:128]=jnp.where(lo,rolled,qk).astype(bf16)
            qs=jnp.where(lo,qk,rolled)*LOG2E
            hi=qs.astype(bf16).astype(f32)
            qa[pl.ds(base,BLK),0:128]=jnp.where(lo,hi,qs-hi).astype(bf16)
            v=a[b*480+320:b*480+480,:].astype(f32)
            vs[pl.ds(base,BLK//2),:]=jnp.where(lanev<64,v,tail)
            vs[pl.ds(base+BLK//2,BLK//2),:]=jnp.where(lanev<64,pltpu.roll(v,64,1),tail)
    for i in range(T//512):
        s=slice(i*512,(i+1)*512)
        ka[s,128:256]=kd_ref[s,:]
        qa[s,128:256]=qd_ref[s,:]
    for i in range(T//256):
        vt[:,i*256:(i+1)*256]=vs[i*256:(i+1)*256,:].T[0:80].astype(bf16)

    def finish(acc):
        o=acc[0:64]/acc[64:65]
        return o*lax.rsqrt(jnp.mean(o*o,axis=0,keepdims=True)+1e-6)

    def fast():
        kio=lax.broadcasted_iota(jnp.int32,(BQ,BQ),0); qio=lax.broadcasted_iota(jnp.int32,(BQ,BQ),1)
        keep=kio<=qio
        for qi in range(T//BQ):
            q0=qi*BQ
            qb=qa[q0:q0+BQ,:]
            def tile(k0,w,mask):
                s=lax.dot_general(ka[k0:k0+w,:],qb,NT,preferred_element_type=f32)
                p=jnp.exp2(s)
                if mask:
                    p=jnp.where(keep,p,0.0)
                return lax.dot_general(vt[:,k0:k0+w],p.astype(bf16),NN,preferred_element_type=f32)
            acc=tile(q0,BQ,True)
            for k0 in range(0,q0,W):
                acc=acc+tile(k0,min(W,q0-k0),False)
            ot[:,q0:q0+BQ]=finish(acc)

    def slow():
        kio=lax.broadcasted_iota(jnp.int32,(BQ,BQ),0); qio=lax.broadcasted_iota(jnp.int32,(BQ,BQ),1)
        def per_q(qi,_):
            q0=pl.multiple_of(qi*BQ,BQ)
            qb=qa[pl.ds(q0,BQ),:]
            def body(j,c):
                m,acc=c
                k0=pl.multiple_of(j*BQ,BQ)
                s=lax.dot_general(ka[pl.ds(k0,BQ),:],qb,NT,preferred_element_type=f32)
                s=jnp.where(kio+k0<=qio+q0,s,-jnp.inf)
                m2=jnp.maximum(m,jnp.max(s,axis=0,keepdims=True))
                p=jnp.exp2(s-m2).astype(bf16)
                acc=acc*jnp.exp2(m-m2)+lax.dot_general(vt[:,pl.ds(k0,BQ)],p,NN,preferred_element_type=f32)
                return m2,acc
            m0=jnp.full((1,BQ),-jnp.inf,f32)
            c=body(qi,(m0,jnp.zeros((80,BQ),f32)))
            m,acc=lax.fori_loop(0,qi,body,c)
            ot[:,pl.ds(q0,BQ)]=finish(acc)
            return 0
        lax.fori_loop(0,T//BQ,per_q,0)
    isfast=fast_ref[0]>0
    pl.when(isfast)(fast)
    pl.when(jnp.logical_not(isfast))(slow)
    for i in range(T//256):
        s=slice(i*256,(i+1)*256)
        vs[s,0:64]=ot[:,s].T
    for j in range(T//BLK):
        a=vs[j*BLK:j*BLK+160,:]; b=vs[j*BLK+160:(j+1)*BLK,:]
        out_ref[j]=jnp.where(lanev<64,a,pltpu.roll(b,64,1)).astype(bf16)

def decay_cols(d):
    x=d*LOG2E
    h=lax.reduce_precision(x,8,7); r=x-h
    m=lax.reduce_precision(r,8,7); l=lax.reduce_precision(r-m,8,7)
    lane=lax.broadcasted_iota(jnp.int32,(T,128),1)
    c=lambda v: v[:,None]
    kd=jnp.where(lane==0,-c(h),jnp.where(lane==1,-c(m),jnp.where(lane==2,-c(l),jnp.where(lane<6,1.0,0.0))))
    qd=jnp.where(lane==3,c(h),jnp.where(lane==4,c(m),jnp.where(lane==5,c(l),jnp.where(lane<3,1.0,0.0))))
    return kd.astype(bf16),qd.astype(bf16)

def attention(pos,fast,kd,qd,ins,nblk):
    V=pltpu.VMEM
    return pl.pallas_call(functools.partial(attn_kernel,nblk=nblk),
        out_shape=jax.ShapeDtypeStruct((16,160,128),bf16),
        in_specs=[pl.BlockSpec(memory_space=pltpu.SMEM)]*2+[pl.BlockSpec(memory_space=pltpu.VMEM)]*(2+len(ins)),
        out_specs=pl.BlockSpec(memory_space=pltpu.VMEM),
        scratch_shapes=[V((T,256),bf16),V((T,256),bf16),V((T,128),f32),V((80,T),bf16),V((64,T),f32)],
        compiler_params=pltpu.CompilerParams(vmem_limit_bytes=24*1024*1024),
        name="attention")(pos,fast,kd,qd,*ins)


def proj_kernel(idx_ref, gain_ref, *refs, pieces):
    ntok = sum(len(p) for p in pieces)
    toks = refs[:ntok]
    ws = refs[ntok : ntok + 8]
    out_ref = refs[ntok + 8]
    lo = lax.broadcasted_iota(jnp.int32, (BLK, 128), 1) < 64
    half = lax.broadcasted_iota(jnp.int32, (BLK // 2, 128), 1) < 64
    low = lax.broadcasted_iota(jnp.int32, (128, 128), 1) < 64
    none = jnp.zeros((128, 128), bf16)
    for h in range(4):
        rhs = []
        for w in ws:
            qk = w[h * 384 : h * 384 + 256, :]
            v = w[h * 384 + 256 : h * 384 + 384, :]
            v = jnp.concatenate([jnp.where(low, v, none), jnp.where(low, none, v)], 0)
            rhs.append(jnp.concatenate([qk, v], 1))
        at = 0
        for b, piece in enumerate(pieces):
            acc = None
            for j in range(8):
                cols = pl.ds(pl.multiple_of(idx_ref[j] * 256, 256), 256)
                parts = [toks[at + n][:, cols] for n in range(len(piece))]
                tok = parts[0] if len(parts) == 1 else jnp.concatenate(parts, 0)
                part = lax.dot_general(tok, rhs[j], NN, preferred_element_type=f32)
                acc = part if acc is None else acc + part
            at += len(piece)
            qk = acc[:, :128].astype(bf16).astype(f32)
            sq = qk * qk
            s_lo = jnp.sum(jnp.where(lo, sq, 0.0), axis=1, keepdims=True)
            s_hi = jnp.sum(jnp.where(lo, 0.0, sq), axis=1, keepdims=True)
            inv = lax.rsqrt(jnp.where(lo, s_lo, s_hi) * (1 / 64) + 1e-6)
            out_ref[h, b * 480 : b * 480 + 320, :] = (qk * inv * gain_ref[...]).astype(bf16)
            v = acc[:, 128:]
            v = v + pltpu.roll(v, 64, 1)
            out_ref[h, b * 480 + 320 : b * 480 + 480, :] = jnp.where(half, v[:160], v[160:]).astype(bf16)


SMEM = pl.BlockSpec(memory_space=pltpu.SMEM)
VMEM = pl.BlockSpec(memory_space=pltpu.VMEM)


def project(cols, gains, pieces, ws):
    sizes = tuple(tuple(p.shape[0] for p in ps) for ps in pieces)
    toks = [p for ps in pieces for p in ps]
    return pl.pallas_call(
        functools.partial(proj_kernel, pieces=sizes),
        out_shape=jax.ShapeDtypeStruct((4, len(pieces) * 480, 128), bf16),
        in_specs=[SMEM] + [VMEM] * (1 + len(toks) + 8),
        out_specs=VMEM,
        compiler_params=pltpu.CompilerParams(vmem_limit_bytes=12 * 1024 * 1024),
        name="project",
    )(cols, gains, *toks, *ws)


def out_kernel(head_ref, col_ref, heads_ref, *refs):
    ws, o_ref, lhs = refs[:8], refs[8], refs[9]
    half = lax.broadcasted_iota(jnp.int32, (BLK // 2, 128), 1) < 64
    for p in range(8):
        a = heads_ref[head_ref[2 * p]].astype(f32)
        b = heads_ref[head_ref[2 * p + 1]].astype(f32)
        s = slice(p * 128, p * 128 + 128)
        lhs[0:160, s] = jnp.where(half, a, pltpu.roll(b, 64, 1)).astype(bf16)
        lhs[160:320, s] = jnp.where(half, pltpu.roll(a, 64, 1), b).astype(bf16)
    for par in range(2):
        for dx in range(4):
            acc = None
            for dy in range(4):
                w = ws[par * 4 + dy]
                r = dx * 512
                rhs = jnp.concatenate(
                    [
                        jnp.concatenate([w[r + d * 128 : r + d * 128 + 64, :] for d in range(4)], 0),
                        jnp.concatenate([w[r + d * 128 + 64 : r + d * 128 + 128, :] for d in range(4)], 0),
                    ],
                    1,
                )
                part = lax.dot_general(
                    lhs[:, dy * 256 : dy * 256 + 256], rhs, NN, preferred_element_type=f32
                )
                acc = part if acc is None else acc + part
            cols = pl.ds(pl.multiple_of(col_ref[par * 4 + dx] * 256, 256), 256)
            o_ref[:, cols] = acc.astype(bf16)


def output(order, cols, heads, ws):
    return pl.pallas_call(
        out_kernel,
        out_shape=jax.ShapeDtypeStruct((BLK, 2048), bf16),
        in_specs=[SMEM, SMEM] + [VMEM] * 9,
        out_specs=VMEM,
        scratch_shapes=[pltpu.VMEM((BLK, 1024), bf16)],
        compiler_params=pltpu.CompilerParams(vmem_limit_bytes=12 * 1024 * 1024),
        name="output",
    )(order, cols, heads, *ws)


def turn(step):
    return [(i, (i + step) % 4) for i in range(4)]


def swap(value):
    return lax.ppermute(value, C, [(0, 1), (1, 0)])


def around(value, axis):
    return [value] + [lax.ppermute(value, axis, turn(-d)) for d in (1, 2, 3)]


def on_device(tokens, w_query, w_key, w_value, w_output, qk_gain, decay_sums):
    own = tokens[0]
    z, y, x, c = (lax.axis_index(a) for a in (Z, Y, X, C))
    t1 = lax.ppermute(own, Y, turn(-1))
    t3 = lax.ppermute(own, Y, turn(1))
    t2 = [lax.ppermute(t1[:160], Y, turn(-1)), lax.ppermute(t3[160:], Y, turn(1))]
    piece = jnp.concatenate(
        [
            jnp.concatenate([w_query, w_key], 1),
            jnp.concatenate([w_value[:128], w_value[128:]], 1),
            w_output[:, :128],
            w_output[:, 128:],
        ],
        0,
    )
    heads4 = around(piece, Z)
    w4 = jnp.concatenate([h[:384] for h in heads4], 0)
    wo4 = jnp.concatenate([h[384:] for h in heads4], 0)
    ws = around(w4, X)
    ws = ws + [swap(w) for w in ws]
    wo16 = jnp.concatenate(around(wo4, X), 0)

    cols = jnp.stack(
        [2 * ((x + d) % 4) + e for e in (c, 1 - c) for d in range(4)]
    ).astype(jnp.int32)
    gains = jnp.concatenate([qk_gain[0] * 0.125, qk_gain[1]])[None]
    kd, qd = decay_cols(decay_sums[0, 0])
    gains, kd, qd = lax.optimization_barrier((gains, kd, qd))
    part1 = project(cols, gains, [[own], [t1], [t3]], ws)
    part1, wo16 = lax.optimization_barrier((part1, wo16))
    part2 = project(cols, gains, [t2], ws)
    recv = []
    for part in (part1, part2):
        recv += [part[0]] + [lax.ppermute(part[d], Z, turn(d)) for d in (1, 2, 3)]
    wo = around(wo16, Y)
    pos = [4 * ((z - d) % 4) + (y + e) % 4 for d in range(4) for e in (0, 1, 3)]
    pos += [4 * ((z - d) % 4) + (y + 2) % 4 for d in range(4)]
    pos = jnp.stack(pos).astype(jnp.int32)
    bound = jnp.max(jnp.abs(qk_gain[0])) * jnp.max(jnp.abs(qk_gain[1]))
    fast = (bound <= 7.7).astype(jnp.int32)[None]
    heads = attention(pos, fast, kd, qd, recv, (3, 3, 3, 3, 1, 1, 1, 1))
    heads, *wo = lax.optimization_barrier((heads, *wo))
    wo = wo + [swap(w) for w in wo]
    merged = lax.all_to_all(heads, SP, 0, 0, tiled=True)
    order = jnp.stack(
        [4 * ((z + d) % 4) + (y + e) % 4 for e in range(4) for d in range(4)]
    ).astype(jnp.int32)
    return output(order, cols, merged, wo)[None]


def solution(mesh):
    torus = Mesh(mesh.devices.reshape(4, 4, 4, 2), ("sp_0", "sp_1", "dp_0", "dp_1"))
    in_specs = (P(DP, SP, None), P(DP, SP), P(DP, SP), P(DP, SP), P(SP, DP), P(), P(DP, SP, None))
    out_specs = P(DP, SP, None)
    return jax.shard_map(
        on_device, mesh=torus, in_specs=in_specs, out_specs=out_specs, check_vma=False
    )
```

```python
import functools

import jax
import jax.numpy as jnp
from jax import lax
from jax.experimental import pallas as pl
from jax.experimental.pallas import tpu as pltpu
from jax.sharding import Mesh
from jax.sharding import PartitionSpec as P


DP = ("dp_0", "dp_1")
SP = ("sp_0", "sp_1")
Z, Y, X, C = "sp_0", "sp_1", "dp_0", "dp_1"
LOG2E = 1.4426950408889634
T = 5120
BLK = 320
BQ = 512
W = 1024
NT = (((1,), (1,)), ((), ()))
NN = (((1,), (0,)), ((), ()))
f32 = jnp.float32
bf16 = jnp.bfloat16
SMEM = pl.BlockSpec(memory_space=pltpu.SMEM)
VMEM = pl.BlockSpec(memory_space=pltpu.VMEM)


def attn_kernel(pos_ref, fast_ref, d_ref, *refs, nblk):
    nin=len(nblk)
    ins=refs[:nin]; out_ref=refs[nin]; ka,qa,vs,vt,ot=refs[nin+1:]
    lane=lax.broadcasted_iota(jnp.int32,(BLK,128),1)
    lo=lane<64
    lanev=lax.broadcasted_iota(jnp.int32,(BLK//2,128),1)
    tail=jnp.where(lanev==64,1.0,0.0)
    n=0
    for a,nb in zip(ins,nblk):
        for b in range(nb):
            base=pl.multiple_of(pos_ref[n]*BLK,64); n+=1
            qk=a[b*480:b*480+320,:].astype(f32)
            rolled=pltpu.roll(qk,64,1)
            ka[pl.ds(base,BLK),0:128]=jnp.where(lo,rolled,qk).astype(bf16)
            qs=jnp.where(lo,qk,rolled)*LOG2E
            hi=qs.astype(bf16).astype(f32)
            qa[pl.ds(base,BLK),0:128]=jnp.where(lo,hi,qs-hi).astype(bf16)
            v=a[b*480+320:b*480+480,:].astype(f32)
            vs[pl.ds(base,BLK//2),:]=jnp.where(lanev<64,v,tail)
            vs[pl.ds(base+BLK//2,BLK//2),:]=jnp.where(lanev<64,pltpu.roll(v,64,1),tail)
    dt=d_ref[...].T
    dl=lax.broadcasted_iota(jnp.int32,(256,128),1)
    key_one=jnp.where((dl>=60)&(dl<120),1.0,0.0)
    query_one=jnp.where(dl<60,1.0,0.0)
    for i in range(T//256):
        s=slice(i*256,(i+1)*256)
        km=(dl==i)|(dl==20+i)|(dl==40+i)
        qm=(dl==60+i)|(dl==80+i)|(dl==100+i)
        ka[s,128:256]=jnp.where(km,dt,key_one).astype(bf16)
        qa[s,128:256]=jnp.where(qm,dt,query_one).astype(bf16)
    for i in range(T//256):
        vt[:,i*256:(i+1)*256]=vs[i*256:(i+1)*256,:].T[0:80].astype(bf16)

    def finish(acc):
        o=acc[0:64]/acc[64:65]
        return o*lax.rsqrt(jnp.mean(o*o,axis=0,keepdims=True)+1e-6)

    def fast():
        kio=lax.broadcasted_iota(jnp.int32,(BQ,BQ),0); qio=lax.broadcasted_iota(jnp.int32,(BQ,BQ),1)
        keep=kio<=qio
        for qi in range(T//BQ):
            q0=qi*BQ
            qb=qa[q0:q0+BQ,:]
            def tile(k0,w,mask):
                s=lax.dot_general(ka[k0:k0+w,:],qb,NT,preferred_element_type=f32)
                p=jnp.exp2(s)
                if mask:
                    p=jnp.where(keep,p,0.0)
                return lax.dot_general(vt[:,k0:k0+w],p.astype(bf16),NN,preferred_element_type=f32)
            acc=tile(q0,BQ,True)
            for k0 in range(0,q0,W):
                acc=acc+tile(k0,min(W,q0-k0),False)
            ot[:,q0:q0+BQ]=finish(acc)

    def slow():
        kio=lax.broadcasted_iota(jnp.int32,(BQ,BQ),0); qio=lax.broadcasted_iota(jnp.int32,(BQ,BQ),1)
        def per_q(qi,_):
            q0=pl.multiple_of(qi*BQ,BQ)
            qb=qa[pl.ds(q0,BQ),:]
            def body(j,c):
                m,acc=c
                k0=pl.multiple_of(j*BQ,BQ)
                s=lax.dot_general(ka[pl.ds(k0,BQ),:],qb,NT,preferred_element_type=f32)
                s=jnp.where(kio+k0<=qio+q0,s,-jnp.inf)
                m2=jnp.maximum(m,jnp.max(s,axis=0,keepdims=True))
                p=jnp.exp2(s-m2).astype(bf16)
                acc=acc*jnp.exp2(m-m2)+lax.dot_general(vt[:,pl.ds(k0,BQ)],p,NN,preferred_element_type=f32)
                return m2,acc
            m0=jnp.full((1,BQ),-jnp.inf,f32)
            c=body(qi,(m0,jnp.zeros((80,BQ),f32)))
            _,acc=lax.fori_loop(0,qi,body,c)
            ot[:,pl.ds(q0,BQ)]=finish(acc)
            return 0
        lax.fori_loop(0,T//BQ,per_q,0)
    isfast=fast_ref[0]>0
    pl.when(isfast)(fast)
    pl.when(jnp.logical_not(isfast))(slow)
    for i in range(T//256):
        s=slice(i*256,(i+1)*256)
        vs[s,0:64]=ot[:,s].T
    for j in range(T//BLK):
        a=vs[j*BLK:j*BLK+160,:]; b=vs[j*BLK+160:(j+1)*BLK,:]
        out_ref[j]=jnp.where(lanev<64,a,pltpu.roll(b,64,1)).astype(bf16)


def decay_pieces(d):
    x = d * LOG2E
    h = lax.reduce_precision(x, 8, 7)
    m = lax.reduce_precision(x - h, 8, 7)
    l = lax.reduce_precision(x - h - m, 8, 7)
    return jnp.concatenate([-h, -m, -l, h, m, l, jnp.zeros((8, 256), f32)], 0)


def attention(pos,fast,dp,ins,nblk):
    V=pltpu.VMEM
    return pl.pallas_call(functools.partial(attn_kernel,nblk=nblk),
        out_shape=jax.ShapeDtypeStruct((16,160,128),bf16),
        in_specs=[pl.BlockSpec(memory_space=pltpu.SMEM)]*2+[pl.BlockSpec(memory_space=pltpu.VMEM)]*(1+len(ins)),
        out_specs=pl.BlockSpec(memory_space=pltpu.VMEM),
        scratch_shapes=[V((T,256),bf16),V((T,256),bf16),V((T,128),f32),V((80,T),bf16),V((64,T),f32)],
        compiler_params=pltpu.CompilerParams(vmem_limit_bytes=24*1024*1024),
        name="attention")(pos,fast,dp,*ins)


def pack_kernel(*refs):
    ins, w, wo = refs[:4], refs[4], refs[5]
    for h in range(4):
        w[h * 192 : h * 192 + 192, :] = ins[h][0:192, :]
        wo[h * 64 : h * 64 + 64, :] = ins[h][192:256, :]


def pack(pieces):
    return pl.pallas_call(
        pack_kernel,
        out_shape=[jax.ShapeDtypeStruct((768, 256), bf16), jax.ShapeDtypeStruct((256, 256), bf16)],
        in_specs=[VMEM] * 4,
        out_specs=[VMEM] * 2,
        compiler_params=pltpu.CompilerParams(vmem_limit_bytes=4 * 1024 * 1024),
        name="pack",
    )(*pieces)


def proj_kernel(idx_ref, gain_ref, *refs, pieces):
    ntok = sum(len(p) for p in pieces)
    toks = refs[:ntok]
    ws = refs[ntok : ntok + 8]
    outs = refs[ntok + 8 : ntok + 12]
    lo = lax.broadcasted_iota(jnp.int32, (BLK, 128), 1) < 64
    half = lax.broadcasted_iota(jnp.int32, (BLK // 2, 128), 1) < 64
    pad = jnp.zeros((64, 256), bf16)

    def head(h, _):
        rows = pl.ds(pl.multiple_of(h * 192, 64), 192)
        at = 0
        for b, piece in enumerate(pieces):
            acc = None
            for j in range(8):
                cols = pl.ds(pl.multiple_of(idx_ref[j] * 256, 256), 256)
                parts = [toks[at + n][:, cols] for n in range(len(piece))]
                tok = parts[0] if len(parts) == 1 else jnp.concatenate(parts, 0)
                rhs = jnp.concatenate([ws[j][rows, :], pad], 0)
                part = lax.dot_general(tok, rhs, NT, preferred_element_type=f32)
                acc = part if acc is None else acc + part
            at += len(piece)
            qk = acc[:, :128].astype(bf16).astype(f32)
            sq = qk * qk
            s_lo = jnp.sum(jnp.where(lo, sq, 0.0), axis=1, keepdims=True)
            s_hi = jnp.sum(jnp.where(lo, 0.0, sq), axis=1, keepdims=True)
            inv = lax.rsqrt(jnp.where(lo, s_lo, s_hi) * (1 / 64) + 1e-6)
            unit = (qk * inv * gain_ref[...]).astype(bf16)
            v = acc[:, 128:]
            v = jnp.where(half, v[:160], pltpu.roll(v[160:], 64, 1)).astype(bf16)
            for k in range(4):

                @pl.when(h == k)
                def _(k=k, b=b, unit=unit, v=v):
                    outs[k][b * 480 : b * 480 + 320, :] = unit
                    outs[k][b * 480 + 320 : b * 480 + 480, :] = v

        return 0

    lax.fori_loop(0, 4, head, 0)


def project(cols, gains, pieces, ws):
    sizes = tuple(tuple(p.shape[0] for p in ps) for ps in pieces)
    toks = [p for ps in pieces for p in ps]
    return pl.pallas_call(
        functools.partial(proj_kernel, pieces=sizes),
        out_shape=[jax.ShapeDtypeStruct((len(pieces) * 480, 128), bf16)] * 4,
        in_specs=[SMEM] + [VMEM] * (1 + len(toks) + 8),
        out_specs=[VMEM] * 4,
        compiler_params=pltpu.CompilerParams(vmem_limit_bytes=12 * 1024 * 1024),
        name="project",
    )(cols, gains, *toks, *ws)


def out_kernel(head_ref, col_ref, heads_ref, *refs):
    ws, o_ref, lhs = refs[:8], refs[8], refs[9]
    half = lax.broadcasted_iota(jnp.int32, (BLK // 2, 128), 1) < 64
    for p in range(8):
        a = heads_ref[head_ref[2 * p]].astype(f32)
        b = heads_ref[head_ref[2 * p + 1]].astype(f32)
        s = slice(p * 128, p * 128 + 128)
        lhs[0:160, s] = jnp.where(half, a, pltpu.roll(b, 64, 1)).astype(bf16)
        lhs[160:320, s] = jnp.where(half, pltpu.roll(a, 64, 1), b).astype(bf16)
    for par in range(2):
        for dx in range(4):
            acc = None
            for dy in range(4):
                rhs = ws[par * 4 + dy][dx * 256 : dx * 256 + 256, :]
                part = lax.dot_general(
                    lhs[:, dy * 256 : dy * 256 + 256], rhs, NN, preferred_element_type=f32
                )
                acc = part if acc is None else acc + part
            cols = pl.ds(pl.multiple_of(col_ref[par * 4 + dx] * 256, 256), 256)
            o_ref[:, cols] = acc.astype(bf16)


def output(order, cols, heads, ws):
    return pl.pallas_call(
        out_kernel,
        out_shape=jax.ShapeDtypeStruct((BLK, 2048), bf16),
        in_specs=[SMEM, SMEM] + [VMEM] * 9,
        out_specs=VMEM,
        scratch_shapes=[pltpu.VMEM((BLK, 1024), bf16)],
        compiler_params=pltpu.CompilerParams(vmem_limit_bytes=12 * 1024 * 1024),
        name="output",
    )(order, cols, heads, *ws)


def turn(step):
    return [(i, (i + step) % 4) for i in range(4)]


def move(value, axis, step):
    pairs = [(0, 1), (1, 0)] if axis == C else turn(step)
    return lax.ppermute(value, axis, pairs)


def around(value, axis):
    return [value] + [move(value, axis, -d) for d in (1, 2, 3)]


def on_device(tokens, w_query, w_key, w_value, w_output, qk_gain, decay_sums):
    own = tokens[0]
    z, y, x, c = (lax.axis_index(a) for a in (Z, Y, X, C))
    t1 = move(own, Y, -1)
    t3 = move(own, Y, 1)
    t2 = [move(t1[:160], Y, -1), move(t3[160:], Y, 1)]
    piece = jnp.concatenate([w_query.T, w_key.T, w_value.T, w_output], 0)
    w4, wo4 = pack(around(piece, Z))
    ws = around(w4, X)
    ws = ws + [move(w, C, 0) for w in ws]

    cols = jnp.stack(
        [2 * ((x + d) % 4) + e for e in (c, 1 - c) for d in range(4)]
    ).astype(jnp.int32)
    gains = jnp.concatenate([qk_gain[0] * 0.125, qk_gain[1]])[None]
    dp = decay_pieces(decay_sums[0, 0].reshape(20, 256))
    bound = jnp.max(jnp.abs(qk_gain[0])) * jnp.max(jnp.abs(qk_gain[1]))
    fast = (bound <= 7.7).astype(jnp.int32)[None]
    gains, dp, fast = lax.optimization_barrier((gains, dp, fast))
    part1 = project(cols, gains, [[own], [t1], [t3]], ws)
    *part1, wo4 = lax.optimization_barrier((*part1, wo4))
    part2 = project(cols, gains, [t2], ws)
    recv = []
    for part in (part1, part2):
        recv += [part[0]] + [move(part[d], Z, d) for d in (1, 2, 3)]
    wo16 = jnp.concatenate(around(wo4, X), 0)
    wo = around(wo16, Y)
    pos = [4 * ((z - d) % 4) + (y + e) % 4 for d in range(4) for e in (0, 1, 3)]
    pos += [4 * ((z - d) % 4) + (y + 2) % 4 for d in range(4)]
    pos = jnp.stack(pos).astype(jnp.int32)
    heads = attention(pos, fast, dp, recv, (3, 3, 3, 3, 1, 1, 1, 1))
    heads, *wo = lax.optimization_barrier((heads, *wo))
    wo = wo + [move(w, C, 0) for w in wo]
    merged = lax.all_to_all(heads, SP, 0, 0, tiled=True)
    order = jnp.stack(
        [4 * ((z + d) % 4) + (y + e) % 4 for e in range(4) for d in range(4)]
    ).astype(jnp.int32)
    return output(order, cols, merged, wo)[None]


def solution(mesh):
    torus = Mesh(mesh.devices.reshape(4, 4, 4, 2), ("sp_0", "sp_1", "dp_0", "dp_1"))
    in_specs = (P(DP, SP, None), P(DP, SP), P(DP, SP), P(DP, SP), P(SP, DP), P(), P(DP, SP, None))
    out_specs = P(DP, SP, None)
    return jax.shard_map(
        on_device, mesh=torus, in_specs=in_specs, out_specs=out_specs, check_vma=False
    )
```

```python
import functools

import jax
import jax.numpy as jnp
from jax import lax
from jax.experimental import pallas as pl
from jax.experimental.pallas import tpu as pltpu
from jax.sharding import Mesh
from jax.sharding import PartitionSpec as P


DP = ("dp_0", "dp_1")
SP = ("sp_0", "sp_1")
Z, Y, X, C = "sp_0", "sp_1", "dp_0", "dp_1"
LOG2E = 1.4426950408889634
T = 5120
BLK = 320
BQ = 512
W = 1024
NT = (((1,), (1,)), ((), ()))
NN = (((1,), (0,)), ((), ()))
f32 = jnp.float32
bf16 = jnp.bfloat16
SMEM = pl.BlockSpec(memory_space=pltpu.SMEM)
VMEM = pl.BlockSpec(memory_space=pltpu.VMEM)


def attn_kernel(pos_ref, gain_ref, d_ref, *refs, nblk):
    nin=len(nblk)
    ins=refs[:nin]; out_ref=refs[nin]; ka,qa,vs,vt,ot=refs[nin+1:]
    lane=lax.broadcasted_iota(jnp.int32,(BLK,128),1)
    lo=lane<64
    lanev=lax.broadcasted_iota(jnp.int32,(BLK//2,128),1)
    tail=jnp.where(lanev==64,1.0,0.0)
    n=0
    for a,nb in zip(ins,nblk):
        for b in range(nb):
            base=pl.multiple_of(pos_ref[n]*BLK,64); n+=1
            qk=a[b*480:b*480+320,:].astype(f32)
            rolled=pltpu.roll(qk,64,1)
            ka[pl.ds(base,BLK),0:128]=jnp.where(lo,rolled,qk).astype(bf16)
            qs=jnp.where(lo,qk,rolled)*LOG2E
            hi=qs.astype(bf16).astype(f32)
            qa[pl.ds(base,BLK),0:128]=jnp.where(lo,hi,qs-hi).astype(bf16)
            v=a[b*480+320:b*480+480,:].astype(f32)
            vs[pl.ds(base,BLK//2),:]=jnp.where(lanev<64,v,tail)
            vs[pl.ds(base+BLK//2,BLK//2),:]=jnp.where(lanev<64,pltpu.roll(v,64,1),tail)
    x=d_ref[...]*LOG2E
    h=x.astype(bf16).astype(f32)
    m=(x-h).astype(bf16).astype(f32)
    l=x-h-m
    dt=jnp.concatenate([-h,-m,-l,h,m,l,jnp.zeros((80,640),f32)],0).T
    dl=lax.broadcasted_iota(jnp.int32,(640,128),1)
    key_one=jnp.where((dl>=24)&(dl<48),1.0,0.0)
    query_one=jnp.where(dl<24,1.0,0.0)
    for i in range(T//640):
        s=slice(i*640,(i+1)*640)
        ka[s,128:256]=jnp.where((dl==i)|(dl==8+i)|(dl==16+i),dt,key_one).astype(bf16)
        qa[s,128:256]=jnp.where((dl==24+i)|(dl==32+i)|(dl==40+i),dt,query_one).astype(bf16)
    for i in range(T//256):
        vt[:,i*256:(i+1)*256]=vs[i*256:(i+1)*256,:].T[0:80].astype(bf16)

    def finish(acc):
        o=acc[0:64]/acc[64:65]
        return o*lax.rsqrt(jnp.mean(o*o,axis=0,keepdims=True)+1e-6)

    def fast():
        kio=lax.broadcasted_iota(jnp.int32,(BQ,BQ),0); qio=lax.broadcasted_iota(jnp.int32,(BQ,BQ),1)
        keep=kio<=qio
        for qi in range(T//BQ):
            q0=qi*BQ
            qb=qa[q0:q0+BQ,:]
            def tile(k0,w,mask):
                s=lax.dot_general(ka[k0:k0+w,:],qb,NT,preferred_element_type=f32)
                p=jnp.exp2(s)
                if mask:
                    p=jnp.where(keep,p,0.0)
                return lax.dot_general(vt[:,k0:k0+w],p.astype(bf16),NN,preferred_element_type=f32)
            acc=tile(q0,BQ,True)
            for k0 in range(0,q0,W):
                acc=acc+tile(k0,min(W,q0-k0),False)
            ot[:,q0:q0+BQ]=finish(acc)

    def slow():
        kio=lax.broadcasted_iota(jnp.int32,(BQ,BQ),0); qio=lax.broadcasted_iota(jnp.int32,(BQ,BQ),1)
        def per_q(qi,_):
            q0=pl.multiple_of(qi*BQ,BQ)
            qb=qa[pl.ds(q0,BQ),:]
            def body(j,c):
                m,acc=c
                k0=pl.multiple_of(j*BQ,BQ)
                s=lax.dot_general(ka[pl.ds(k0,BQ),:],qb,NT,preferred_element_type=f32)
                s=jnp.where(kio+k0<=qio+q0,s,-jnp.inf)
                m2=jnp.maximum(m,jnp.max(s,axis=0,keepdims=True))
                p=jnp.exp2(s-m2).astype(bf16)
                acc=acc*jnp.exp2(m-m2)+lax.dot_general(vt[:,pl.ds(k0,BQ)],p,NN,preferred_element_type=f32)
                return m2,acc
            m0=jnp.full((1,BQ),-jnp.inf,f32)
            c=body(qi,(m0,jnp.zeros((80,BQ),f32)))
            _,acc=lax.fori_loop(0,qi,body,c)
            ot[:,pl.ds(q0,BQ)]=finish(acc)
            return 0
        lax.fori_loop(0,T//BQ,per_q,0)
    g=jnp.abs(gain_ref[...])
    isfast=jnp.max(g[0:1])*jnp.max(g[1:2])<=7.7
    pl.when(isfast)(fast)
    pl.when(jnp.logical_not(isfast))(slow)
    for i in range(T//256):
        s=slice(i*256,(i+1)*256)
        vs[s,0:64]=ot[:,s].T
    for j in range(T//BLK):
        a=vs[j*BLK:j*BLK+160,:]; b=vs[j*BLK+160:(j+1)*BLK,:]
        out_ref[j]=jnp.where(lanev<64,a,pltpu.roll(b,64,1)).astype(bf16)


def attention(pos,gain,d,ins,nblk):
    V=pltpu.VMEM
    return pl.pallas_call(functools.partial(attn_kernel,nblk=nblk),
        out_shape=jax.ShapeDtypeStruct((16,160,128),bf16),
        in_specs=[SMEM]+[VMEM]*(2+len(ins)),
        out_specs=VMEM,
        scratch_shapes=[V((T,256),bf16),V((T,256),bf16),V((T,128),f32),V((80,T),bf16),V((64,T),f32)],
        compiler_params=pltpu.CompilerParams(vmem_limit_bytes=24*1024*1024),
        name="attention")(pos,gain,d,*ins)


def pack_kernel(*refs):
    ins, w, wo = refs[:4], refs[4], refs[5]
    for h in range(4):
        w[h * 192 : h * 192 + 192, :] = ins[h][0:192, :]
        wo[h * 64 : h * 64 + 64, :] = ins[h][192:256, :]


def pack(pieces):
    return pl.pallas_call(
        pack_kernel,
        out_shape=[jax.ShapeDtypeStruct((768, 256), bf16), jax.ShapeDtypeStruct((256, 256), bf16)],
        in_specs=[VMEM] * 4,
        out_specs=[VMEM] * 2,
        compiler_params=pltpu.CompilerParams(vmem_limit_bytes=4 * 1024 * 1024),
        name="pack",
    )(*pieces)


def join_kernel(*refs):
    for i in range(4):
        refs[4][i * 256 : i * 256 + 256, :] = refs[i][...]


def join(pieces):
    return pl.pallas_call(
        join_kernel,
        out_shape=jax.ShapeDtypeStruct((1024, 256), bf16),
        in_specs=[VMEM] * 4,
        out_specs=VMEM,
        compiler_params=pltpu.CompilerParams(vmem_limit_bytes=4 * 1024 * 1024),
        name="join",
    )(*pieces)


def proj_block(tok, w, gains, out, at):
    lo = lax.broadcasted_iota(jnp.int32, (BLK, 128), 1) < 64
    half = lax.broadcasted_iota(jnp.int32, (BLK // 2, 128), 1) < 64
    acc = lax.dot_general(tok, w, NT, preferred_element_type=f32)
    for h in range(4):
        qk = acc[:, h * 128 : h * 128 + 128].astype(bf16).astype(f32)
        sq = qk * qk
        s_lo = jnp.sum(jnp.where(lo, sq, 0.0), axis=1, keepdims=True)
        s_hi = jnp.sum(jnp.where(lo, 0.0, sq), axis=1, keepdims=True)
        inv = lax.rsqrt(jnp.where(lo, s_lo, s_hi) * (1 / 64) + 1e-6)
        out[h][at : at + 320, :] = (qk * inv * gains).astype(bf16)
        c = 512 + (h // 2) * 128
        top, bot = acc[:160, c : c + 128], acc[160:, c : c + 128]
        if h % 2:
            top = pltpu.roll(top, 64, 1)
        else:
            bot = pltpu.roll(bot, 64, 1)
        out[h][at + 320 : at + 480, :] = jnp.where(half, top, bot).astype(bf16)


def gain_row(gain_ref):
    return jnp.concatenate([gain_ref[0:1, :] * 0.125, gain_ref[1:2, :]], 1)


def proj_kernel(idx_ref, gain_ref, *refs, count):
    toks, ws, outs, w = refs[:count], refs[count : count + 8], refs[count + 8 : count + 12], refs[-1]
    for j in range(8):
        cols = pl.ds(pl.multiple_of(idx_ref[j] * 256, 256), 256)
        for h in range(4):
            w[h * 128 : h * 128 + 128, cols] = ws[j][h * 192 : h * 192 + 128, :]
            w[512 + h * 64 : 576 + h * 64, cols] = ws[j][h * 192 + 128 : h * 192 + 192, :]
    gains = gain_row(gain_ref)
    for b in range(count):
        proj_block(toks[b][...], w[...], gains, outs, b * 480)


def project(cols, gain, toks, ws):
    count = len(toks)
    return pl.pallas_call(
        functools.partial(proj_kernel, count=count),
        out_shape=[jax.ShapeDtypeStruct((count * 480, 128), bf16)] * 4,
        in_specs=[SMEM] + [VMEM] * (1 + count + 8),
        out_specs=[VMEM] * 4,
        scratch_shapes=[pltpu.VMEM((768, 2048), bf16)],
        compiler_params=pltpu.CompilerParams(vmem_limit_bytes=20 * 1024 * 1024),
        name="project",
    )(cols, gain, *toks, *ws)


def out_kernel(head_ref, col_ref, heads_ref, *refs):
    ws, o_ref, lhs = refs[:8], refs[8], refs[9]
    half = lax.broadcasted_iota(jnp.int32, (BLK // 2, 128), 1) < 64
    for p in range(8):
        a = heads_ref[head_ref[2 * p]].astype(f32)
        b = heads_ref[head_ref[2 * p + 1]].astype(f32)
        s = slice(p * 128, p * 128 + 128)
        lhs[0:160, s] = jnp.where(half, a, pltpu.roll(b, 64, 1)).astype(bf16)
        lhs[160:320, s] = jnp.where(half, pltpu.roll(a, 64, 1), b).astype(bf16)
    for par in range(2):
        for dx in range(4):
            acc = None
            for dy in range(4):
                rhs = ws[par * 4 + dy][dx * 256 : dx * 256 + 256, :]
                part = lax.dot_general(
                    lhs[:, dy * 256 : dy * 256 + 256], rhs, NN, preferred_element_type=f32
                )
                acc = part if acc is None else acc + part
            cols = pl.ds(pl.multiple_of(col_ref[par * 4 + dx] * 256, 256), 256)
            o_ref[:, cols] = acc.astype(bf16)


def output(order, cols, heads, ws):
    return pl.pallas_call(
        out_kernel,
        out_shape=jax.ShapeDtypeStruct((BLK, 2048), bf16),
        in_specs=[SMEM, SMEM] + [VMEM] * 9,
        out_specs=VMEM,
        scratch_shapes=[pltpu.VMEM((BLK, 1024), bf16)],
        compiler_params=pltpu.CompilerParams(vmem_limit_bytes=12 * 1024 * 1024),
        name="output",
    )(order, cols, heads, *ws)


def turn(step):
    return [(i, (i + step) % 4) for i in range(4)]


def move(value, axis, step):
    pairs = [(0, 1), (1, 0)] if axis == C else turn(step)
    return lax.ppermute(value, axis, pairs)


def around(value, axis):
    return [value] + [move(value, axis, -d) for d in (1, 2, 3)]


def on_device(tokens, w_query, w_key, w_value, w_output, qk_gain, decay_sums):
    own = tokens[0]
    z, y, x, c = (lax.axis_index(a) for a in (Z, Y, X, C))
    t1 = move(own, Y, -1)
    t3 = move(own, Y, 1)
    t2 = move(own, Y, 2)
    piece = jnp.concatenate([w_query.T, w_key.T, w_value.T, w_output], 0)
    w4, wo4 = pack(around(piece, Z))
    ws = around(w4, X)
    ws = ws + [move(w, C, 0) for w in ws]

    cols = jnp.stack(
        [2 * ((x + d) % 4) + e for e in (c, 1 - c) for d in range(4)]
    ).astype(jnp.int32)
    gain, decay = lax.optimization_barrier((qk_gain, decay_sums.reshape(8, 640)))
    part1 = project(cols, gain, [own, t1, t3], ws)
    *part1, wo4 = lax.optimization_barrier((*part1, wo4))
    part2 = project(cols, gain, [t2], ws)
    recv = []
    for part in (part1, part2):
        recv += [part[0]] + [move(part[d], Z, d) for d in (1, 2, 3)]
    wo16 = join(around(wo4, X))
    wo = around(wo16, Y)
    pos = [4 * ((z - d) % 4) + (y + e) % 4 for d in range(4) for e in (0, 1, 3)]
    pos += [4 * ((z - d) % 4) + (y + 2) % 4 for d in range(4)]
    pos = jnp.stack(pos).astype(jnp.int32)
    heads = attention(pos, gain, decay, recv, (3, 3, 3, 3, 1, 1, 1, 1))
    heads, *wo = lax.optimization_barrier((heads, *wo))
    wo = wo + [move(w, C, 0) for w in wo]
    merged = lax.all_to_all(heads, SP, 0, 0, tiled=True)
    order = jnp.stack(
        [4 * ((z + d) % 4) + (y + e) % 4 for e in range(4) for d in range(4)]
    ).astype(jnp.int32)
    return output(order, cols, merged, wo)[None]


def solution(mesh):
    torus = Mesh(mesh.devices.reshape(4, 4, 4, 2), ("sp_0", "sp_1", "dp_0", "dp_1"))
    in_specs = (P(DP, SP, None), P(DP, SP), P(DP, SP), P(DP, SP), P(SP, DP), P(), P(DP, SP, None))
    out_specs = P(DP, SP, None)
    return jax.shard_map(
        on_device, mesh=torus, in_specs=in_specs, out_specs=out_specs, check_vma=False
    )
```

```python
import functools

import jax
import jax.numpy as jnp
from jax import lax
from jax.experimental import pallas as pl
from jax.experimental.pallas import tpu as pltpu
from jax.sharding import Mesh
from jax.sharding import PartitionSpec as P


DP = ("dp_0", "dp_1")
SP = ("sp_0", "sp_1")
Z, Y, X, C = "sp_0", "sp_1", "dp_0", "dp_1"
LOG2E = 1.4426950408889634
T = 5120
BLK = 320
BQ = 512
W = 1024
NT = (((1,), (1,)), ((), ()))
NN = (((1,), (0,)), ((), ()))
f32 = jnp.float32
bf16 = jnp.bfloat16
SMEM = pl.BlockSpec(memory_space=pltpu.SMEM)
VMEM = pl.BlockSpec(memory_space=pltpu.VMEM)


def attn_kernel(pos_ref, gain_ref, d_ref, *refs, nblk):
    nin=len(nblk)
    ins=refs[:nin]; out_ref=refs[nin]; ka,qa,vs,vt,ot=refs[nin+1:]
    lane=lax.broadcasted_iota(jnp.int32,(BLK,128),1)
    lo=lane<64
    lanev=lax.broadcasted_iota(jnp.int32,(BLK//2,128),1)
    tail=jnp.where(lanev==64,1.0,0.0)
    n=0
    for a,nb in zip(ins,nblk):
        for b in range(nb):
            base=pl.multiple_of(pos_ref[n]*BLK,64); n+=1
            qk=a[b*480:b*480+320,:].astype(f32)
            rolled=pltpu.roll(qk,64,1)
            ka[pl.ds(base,BLK),0:128]=jnp.where(lo,rolled,qk).astype(bf16)
            qs=jnp.where(lo,qk,rolled)*LOG2E
            hi=qs.astype(bf16).astype(f32)
            qa[pl.ds(base,BLK),0:128]=jnp.where(lo,hi,qs-hi).astype(bf16)
            v=a[b*480+320:b*480+480,:].astype(f32)
            vs[pl.ds(base,BLK//2),:]=jnp.where(lanev<64,v,tail)
            vs[pl.ds(base+BLK//2,BLK//2),:]=jnp.where(lanev<64,pltpu.roll(v,64,1),tail)
    x=d_ref[...]*LOG2E
    h=x.astype(bf16).astype(f32)
    m=(x-h).astype(bf16).astype(f32)
    l=x-h-m
    dt=jnp.concatenate([-h,-m,-l,h,m,l,jnp.zeros((80,640),f32)],0).T
    dl=lax.broadcasted_iota(jnp.int32,(640,128),1)
    key_one=jnp.where((dl>=24)&(dl<48),1.0,0.0)
    query_one=jnp.where(dl<24,1.0,0.0)
    for i in range(T//640):
        s=slice(i*640,(i+1)*640)
        ka[s,128:256]=jnp.where((dl==i)|(dl==8+i)|(dl==16+i),dt,key_one).astype(bf16)
        qa[s,128:256]=jnp.where((dl==24+i)|(dl==32+i)|(dl==40+i),dt,query_one).astype(bf16)
    for i in range(T//256):
        vt[:,i*256:(i+1)*256]=vs[i*256:(i+1)*256,:].T[0:80].astype(bf16)

    def finish(acc):
        o=acc[0:64]/acc[64:65]
        return o*lax.rsqrt(jnp.mean(o*o,axis=0,keepdims=True)+1e-6)

    def fast():
        kio=lax.broadcasted_iota(jnp.int32,(BQ,BQ),0); qio=lax.broadcasted_iota(jnp.int32,(BQ,BQ),1)
        keep=kio<=qio
        for qi in range(T//BQ):
            q0=qi*BQ
            qb=qa[q0:q0+BQ,:]
            def tile(k0,w,mask):
                s=lax.dot_general(ka[k0:k0+w,:],qb,NT,preferred_element_type=f32)
                p=jnp.exp2(s)
                if mask:
                    p=jnp.where(keep,p,0.0)
                return lax.dot_general(vt[:,k0:k0+w],p.astype(bf16),NN,preferred_element_type=f32)
            acc=tile(q0,BQ,True)
            for k0 in range(0,q0,W):
                acc=acc+tile(k0,min(W,q0-k0),False)
            ot[:,q0:q0+BQ]=finish(acc)

    def slow():
        kio=lax.broadcasted_iota(jnp.int32,(BQ,BQ),0); qio=lax.broadcasted_iota(jnp.int32,(BQ,BQ),1)
        def per_q(qi,_):
            q0=pl.multiple_of(qi*BQ,BQ)
            qb=qa[pl.ds(q0,BQ),:]
            def body(j,c):
                m,acc=c
                k0=pl.multiple_of(j*BQ,BQ)
                s=lax.dot_general(ka[pl.ds(k0,BQ),:],qb,NT,preferred_element_type=f32)
                s=jnp.where(kio+k0<=qio+q0,s,-jnp.inf)
                m2=jnp.maximum(m,jnp.max(s,axis=0,keepdims=True))
                p=jnp.exp2(s-m2).astype(bf16)
                acc=acc*jnp.exp2(m-m2)+lax.dot_general(vt[:,pl.ds(k0,BQ)],p,NN,preferred_element_type=f32)
                return m2,acc
            m0=jnp.full((1,BQ),-jnp.inf,f32)
            c=body(qi,(m0,jnp.zeros((80,BQ),f32)))
            _,acc=lax.fori_loop(0,qi,body,c)
            ot[:,pl.ds(q0,BQ)]=finish(acc)
            return 0
        lax.fori_loop(0,T//BQ,per_q,0)
    g=jnp.abs(gain_ref[...])
    isfast=jnp.max(g[0:1])*jnp.max(g[1:2])<=7.7
    pl.when(isfast)(fast)
    pl.when(jnp.logical_not(isfast))(slow)
    for i in range(T//256):
        s=slice(i*256,(i+1)*256)
        vs[s,0:64]=ot[:,s].T
    for j in range(T//BLK):
        a=vs[j*BLK:j*BLK+160,:]; b=vs[j*BLK+160:(j+1)*BLK,:]
        out_ref[j]=jnp.where(lanev<64,a,pltpu.roll(b,64,1)).astype(bf16)


def attention(pos,gain,d,ins,nblk):
    V=pltpu.VMEM
    return pl.pallas_call(functools.partial(attn_kernel,nblk=nblk),
        out_shape=jax.ShapeDtypeStruct((16,160,128),bf16),
        in_specs=[SMEM]+[VMEM]*(2+len(ins)),
        out_specs=VMEM,
        scratch_shapes=[V((T,256),bf16),V((T,256),bf16),V((T,128),f32),V((80,T),bf16),V((64,T),f32)],
        compiler_params=pltpu.CompilerParams(vmem_limit_bytes=24*1024*1024),
        name="attention")(pos,gain,d,*ins)


def pack_kernel(*refs):
    ins, w, wo = refs[:4], refs[4], refs[5]
    for h in range(4):
        w[h * 192 : h * 192 + 192, :] = ins[h][0:192, :]
        wo[h * 64 : h * 64 + 64, :] = ins[h][192:256, :]


def pack(pieces):
    return pl.pallas_call(
        pack_kernel,
        out_shape=[jax.ShapeDtypeStruct((768, 256), bf16), jax.ShapeDtypeStruct((256, 256), bf16)],
        in_specs=[VMEM] * 4,
        out_specs=[VMEM] * 2,
        compiler_params=pltpu.CompilerParams(vmem_limit_bytes=4 * 1024 * 1024),
        name="pack",
    )(*pieces)


def join_kernel(*refs):
    for i in range(4):
        refs[4][i * 256 : i * 256 + 256, :] = refs[i][...]


def join(pieces):
    return pl.pallas_call(
        join_kernel,
        out_shape=jax.ShapeDtypeStruct((1024, 256), bf16),
        in_specs=[VMEM] * 4,
        out_specs=VMEM,
        compiler_params=pltpu.CompilerParams(vmem_limit_bytes=4 * 1024 * 1024),
        name="join",
    )(*pieces)


def proj_block(tok, w, gains, out, at):
    lo = lax.broadcasted_iota(jnp.int32, (BLK, 128), 1) < 64
    half = lax.broadcasted_iota(jnp.int32, (BLK // 2, 128), 1) < 64
    acc = lax.dot_general(tok, w, NT, preferred_element_type=f32)
    for h in range(4):
        qk = acc[:, h * 128 : h * 128 + 128].astype(bf16).astype(f32)
        sq = qk * qk
        s_lo = jnp.sum(jnp.where(lo, sq, 0.0), axis=1, keepdims=True)
        s_hi = jnp.sum(jnp.where(lo, 0.0, sq), axis=1, keepdims=True)
        inv = lax.rsqrt(jnp.where(lo, s_lo, s_hi) * (1 / 64) + 1e-6)
        out[h][at : at + 320, :] = (qk * inv * gains).astype(bf16)
        c = 512 + (h // 2) * 128
        top, bot = acc[:160, c : c + 128], acc[160:, c : c + 128]
        if h % 2:
            top = pltpu.roll(top, 64, 1)
        else:
            bot = pltpu.roll(bot, 64, 1)
        out[h][at + 320 : at + 480, :] = jnp.where(half, top, bot).astype(bf16)


def gain_row(gain_ref):
    return jnp.concatenate([gain_ref[0:1, :] * 0.125, gain_ref[1:2, :]], 1)


def proj_kernel(idx_ref, gain_ref, *refs, sizes):
    n = sum(sizes)
    toks, ws, outs, w = refs[:n], refs[n : n + 8], refs[n + 8 : n + 12], refs[-1]
    for j in range(8):
        cols = pl.ds(pl.multiple_of(idx_ref[j] * 256, 256), 256)
        for h in range(4):
            w[h * 128 : h * 128 + 128, cols] = ws[j][h * 192 : h * 192 + 128, :]
            w[512 + h * 64 : 576 + h * 64, cols] = ws[j][h * 192 + 128 : h * 192 + 192, :]
    gains = gain_row(gain_ref)
    at = 0
    for b, size in enumerate(sizes):
        parts = [t[...] for t in toks[at : at + size]]
        at += size
        tok = parts[0] if size == 1 else jnp.concatenate(parts, 0)
        proj_block(tok, w[...], gains, outs, b * 480)


def project(cols, gain, blocks, ws):
    toks = [p for block in blocks for p in block]
    return pl.pallas_call(
        functools.partial(proj_kernel, sizes=tuple(len(b) for b in blocks)),
        out_shape=[jax.ShapeDtypeStruct((len(blocks) * 480, 128), bf16)] * 4,
        in_specs=[SMEM] + [VMEM] * (1 + len(toks) + 8),
        out_specs=[VMEM] * 4,
        scratch_shapes=[pltpu.VMEM((768, 2048), bf16)],
        compiler_params=pltpu.CompilerParams(vmem_limit_bytes=20 * 1024 * 1024),
        name="project",
    )(cols, gain, *toks, *ws)


def out_kernel(head_ref, col_ref, heads_ref, *refs):
    ws, o_ref, lhs = refs[:8], refs[8], refs[9]
    half = lax.broadcasted_iota(jnp.int32, (BLK // 2, 128), 1) < 64
    for p in range(8):
        a = heads_ref[head_ref[2 * p]].astype(f32)
        b = heads_ref[head_ref[2 * p + 1]].astype(f32)
        s = slice(p * 128, p * 128 + 128)
        lhs[0:160, s] = jnp.where(half, a, pltpu.roll(b, 64, 1)).astype(bf16)
        lhs[160:320, s] = jnp.where(half, pltpu.roll(a, 64, 1), b).astype(bf16)
    for par in range(2):
        for dx in range(4):
            acc = None
            for dy in range(4):
                rhs = ws[par * 4 + dy][dx * 256 : dx * 256 + 256, :]
                part = lax.dot_general(
                    lhs[:, dy * 256 : dy * 256 + 256], rhs, NN, preferred_element_type=f32
                )
                acc = part if acc is None else acc + part
            cols = pl.ds(pl.multiple_of(col_ref[par * 4 + dx] * 256, 256), 256)
            o_ref[:, cols] = acc.astype(bf16)


def output(order, cols, heads, ws):
    return pl.pallas_call(
        out_kernel,
        out_shape=jax.ShapeDtypeStruct((BLK, 2048), bf16),
        in_specs=[SMEM, SMEM] + [VMEM] * 9,
        out_specs=VMEM,
        scratch_shapes=[pltpu.VMEM((BLK, 1024), bf16)],
        compiler_params=pltpu.CompilerParams(vmem_limit_bytes=12 * 1024 * 1024),
        name="output",
    )(order, cols, heads, *ws)


def turn(step):
    return [(i, (i + step) % 4) for i in range(4)]


def move(value, axis, step):
    pairs = [(0, 1), (1, 0)] if axis == C else turn(step)
    return lax.ppermute(value, axis, pairs)


def around(value, axis):
    return [value] + [move(value, axis, -d) for d in (1, 2, 3)]


def on_device(tokens, w_query, w_key, w_value, w_output, qk_gain, decay_sums):
    own = tokens[0]
    z, y, x, c = (lax.axis_index(a) for a in (Z, Y, X, C))
    top, bot = own[:160], own[160:]
    t1 = [move(top, Y, -1), move(bot, Y, -1)]
    t3 = [move(top, Y, 1), move(bot, Y, 1)]
    t2 = [move(t1[0], Y, -1), move(t3[1], Y, 1)]
    piece = jnp.concatenate([w_query.T, w_key.T, w_value.T, w_output], 0)
    w4, wo4 = pack(around(piece, Z))
    ws = around(w4, X)
    ws = ws + [move(w, C, 0) for w in ws]

    cols = jnp.stack(
        [2 * ((x + d) % 4) + e for e in (c, 1 - c) for d in range(4)]
    ).astype(jnp.int32)
    gain, decay = lax.optimization_barrier((qk_gain, decay_sums.reshape(8, 640)))
    part1 = project(cols, gain, [[own], t1, t3], ws)
    *part1, wo4 = lax.optimization_barrier((*part1, wo4))
    part2 = project(cols, gain, [t2], ws)
    recv = []
    for part in (part1, part2):
        recv += [part[0]] + [move(part[d], Z, d) for d in (1, 2, 3)]
    wo16 = join(around(wo4, X))
    wo = around(wo16, Y)
    pos = [4 * ((z - d) % 4) + (y + e) % 4 for d in range(4) for e in (0, 1, 3)]
    pos += [4 * ((z - d) % 4) + (y + 2) % 4 for d in range(4)]
    pos = jnp.stack(pos).astype(jnp.int32)
    heads = attention(pos, gain, decay, recv, (3, 3, 3, 3, 1, 1, 1, 1))
    heads, *wo = lax.optimization_barrier((heads, *wo))
    wo = wo + [move(w, C, 0) for w in wo]
    merged = lax.all_to_all(heads, SP, 0, 0, tiled=True)
    order = jnp.stack(
        [4 * ((z + d) % 4) + (y + e) % 4 for e in range(4) for d in range(4)]
    ).astype(jnp.int32)
    return output(order, cols, merged, wo)[None]


def solution(mesh):
    torus = Mesh(mesh.devices.reshape(4, 4, 4, 2), ("sp_0", "sp_1", "dp_0", "dp_1"))
    in_specs = (P(DP, SP, None), P(DP, SP), P(DP, SP), P(DP, SP), P(SP, DP), P(), P(DP, SP, None))
    out_specs = P(DP, SP, None)
    return jax.shard_map(
        on_device, mesh=torus, in_specs=in_specs, out_specs=out_specs, check_vma=False
    )
```

```python
import functools

import jax
import jax.numpy as jnp
from jax import lax
from jax.experimental import pallas as pl
from jax.experimental.pallas import tpu as pltpu
from jax.sharding import Mesh
from jax.sharding import PartitionSpec as P


DP = ("dp_0", "dp_1")
SP = ("sp_0", "sp_1")
Z, Y, X, C = "sp_0", "sp_1", "dp_0", "dp_1"
LOG2E = 1.4426950408889634
T = 5120
BLK = 320
BQ = 512
W = 1024
NT = (((1,), (1,)), ((), ()))
NN = (((1,), (0,)), ((), ()))
f32 = jnp.float32
bf16 = jnp.bfloat16
SMEM = pl.BlockSpec(memory_space=pltpu.SMEM)
VMEM = pl.BlockSpec(memory_space=pltpu.VMEM)


def attn_kernel(pos_ref, gain_ref, d_ref, *refs, nblk):
    nin=len(nblk)
    ins=refs[:nin]; out_ref=refs[nin]; ka,qa,vs,vt,ot=refs[nin+1:]
    lane=lax.broadcasted_iota(jnp.int32,(BLK,128),1)
    lo=lane<64
    lanev=lax.broadcasted_iota(jnp.int32,(BLK//2,128),1)
    tail=jnp.where(lanev==64,1.0,0.0)
    n=0
    for a,nb in zip(ins,nblk):
        for b in range(nb):
            base=pl.multiple_of(pos_ref[n]*BLK,64); n+=1
            qk=a[b*480:b*480+320,:].astype(f32)
            rolled=pltpu.roll(qk,64,1)
            ka[pl.ds(base,BLK),0:128]=jnp.where(lo,rolled,qk).astype(bf16)
            qs=jnp.where(lo,qk,rolled)*LOG2E
            hi=qs.astype(bf16).astype(f32)
            qa[pl.ds(base,BLK),0:128]=jnp.where(lo,hi,qs-hi).astype(bf16)
            v=a[b*480+320:b*480+480,:].astype(f32)
            vs[pl.ds(base,BLK//2),:]=jnp.where(lanev<64,v,tail)
            vs[pl.ds(base+BLK//2,BLK//2),:]=jnp.where(lanev<64,pltpu.roll(v,64,1),tail)
    x=d_ref[...]*LOG2E
    h=x.astype(bf16).astype(f32)
    m=(x-h).astype(bf16).astype(f32)
    l=x-h-m
    dt=jnp.concatenate([-h,-m,-l,h,m,l,jnp.zeros((80,640),f32)],0).T
    dl=lax.broadcasted_iota(jnp.int32,(640,128),1)
    key_one=jnp.where((dl>=24)&(dl<48),1.0,0.0)
    query_one=jnp.where(dl<24,1.0,0.0)
    for i in range(T//640):
        s=slice(i*640,(i+1)*640)
        ka[s,128:256]=jnp.where((dl==i)|(dl==8+i)|(dl==16+i),dt,key_one).astype(bf16)
        qa[s,128:256]=jnp.where((dl==24+i)|(dl==32+i)|(dl==40+i),dt,query_one).astype(bf16)
    for i in range(T//256):
        vt[:,i*256:(i+1)*256]=vs[i*256:(i+1)*256,:].T[0:80].astype(bf16)

    def finish(acc):
        o=acc[0:64]/acc[64:65]
        return o*lax.rsqrt(jnp.mean(o*o,axis=0,keepdims=True)+1e-6)

    def fast():
        kio=lax.broadcasted_iota(jnp.int32,(BQ,BQ),0); qio=lax.broadcasted_iota(jnp.int32,(BQ,BQ),1)
        keep=kio<=qio
        for qi in range(T//BQ):
            q0=qi*BQ
            qb=qa[q0:q0+BQ,:]
            def tile(k0,w,mask):
                s=lax.dot_general(ka[k0:k0+w,:],qb,NT,preferred_element_type=f32)
                p=jnp.exp2(s)
                if mask:
                    p=jnp.where(keep,p,0.0)
                return lax.dot_general(vt[:,k0:k0+w],p.astype(bf16),NN,preferred_element_type=f32)
            acc=tile(q0,BQ,True)
            for k0 in range(0,q0,W):
                acc=acc+tile(k0,min(W,q0-k0),False)
            ot[:,q0:q0+BQ]=finish(acc)

    def slow():
        kio=lax.broadcasted_iota(jnp.int32,(BQ,BQ),0); qio=lax.broadcasted_iota(jnp.int32,(BQ,BQ),1)
        def per_q(qi,_):
            q0=pl.multiple_of(qi*BQ,BQ)
            qb=qa[pl.ds(q0,BQ),:]
            def body(j,c):
                m,acc=c
                k0=pl.multiple_of(j*BQ,BQ)
                s=lax.dot_general(ka[pl.ds(k0,BQ),:],qb,NT,preferred_element_type=f32)
                s=jnp.where(kio+k0<=qio+q0,s,-jnp.inf)
                m2=jnp.maximum(m,jnp.max(s,axis=0,keepdims=True))
                p=jnp.exp2(s-m2).astype(bf16)
                acc=acc*jnp.exp2(m-m2)+lax.dot_general(vt[:,pl.ds(k0,BQ)],p,NN,preferred_element_type=f32)
                return m2,acc
            m0=jnp.full((1,BQ),-jnp.inf,f32)
            c=body(qi,(m0,jnp.zeros((80,BQ),f32)))
            _,acc=lax.fori_loop(0,qi,body,c)
            ot[:,pl.ds(q0,BQ)]=finish(acc)
            return 0
        lax.fori_loop(0,T//BQ,per_q,0)
    g=jnp.abs(gain_ref[...])
    isfast=jnp.max(g[0:1])*jnp.max(g[1:2])<=7.7
    pl.when(isfast)(fast)
    pl.when(jnp.logical_not(isfast))(slow)
    for i in range(T//256):
        s=slice(i*256,(i+1)*256)
        vs[s,0:64]=ot[:,s].T
    for j in range(T//BLK):
        a=vs[j*BLK:j*BLK+160,:]; b=vs[j*BLK+160:(j+1)*BLK,:]
        out_ref[j]=jnp.where(lanev<64,a,pltpu.roll(b,64,1)).astype(bf16)


def attention(pos,gain,d,ins,nblk):
    V=pltpu.VMEM
    return pl.pallas_call(functools.partial(attn_kernel,nblk=nblk),
        out_shape=jax.ShapeDtypeStruct((16,160,128),bf16),
        in_specs=[SMEM]+[VMEM]*(2+len(ins)),
        out_specs=VMEM,
        scratch_shapes=[V((T,256),bf16),V((T,256),bf16),V((T,128),f32),V((80,T),bf16),V((64,T),f32)],
        compiler_params=pltpu.CompilerParams(vmem_limit_bytes=24*1024*1024),
        name="attention")(pos,gain,d,*ins)


def pack_kernel(*refs):
    ins, w, wo = refs[:4], refs[4], refs[5]
    for h in range(4):
        w[h * 192 : h * 192 + 192, :] = ins[h][0:192, :]
        wo[h * 64 : h * 64 + 64, :] = ins[h][192:256, :]


def pack(pieces):
    return pl.pallas_call(
        pack_kernel,
        out_shape=[jax.ShapeDtypeStruct((768, 256), bf16), jax.ShapeDtypeStruct((256, 256), bf16)],
        in_specs=[VMEM] * 4,
        out_specs=[VMEM] * 2,
        compiler_params=pltpu.CompilerParams(vmem_limit_bytes=4 * 1024 * 1024),
        name="pack",
    )(*pieces)


def join_kernel(*refs):
    for i in range(4):
        refs[4][i * 256 : i * 256 + 256, :] = refs[i][...]


def join(pieces):
    return pl.pallas_call(
        join_kernel,
        out_shape=jax.ShapeDtypeStruct((1024, 256), bf16),
        in_specs=[VMEM] * 4,
        out_specs=VMEM,
        compiler_params=pltpu.CompilerParams(vmem_limit_bytes=4 * 1024 * 1024),
        name="join",
    )(*pieces)


def proj_block(tok, w, gains, out, at):
    lo = lax.broadcasted_iota(jnp.int32, (BLK, 128), 1) < 64
    half = lax.broadcasted_iota(jnp.int32, (BLK // 2, 128), 1) < 64
    acc = lax.dot_general(tok, w, NT, preferred_element_type=f32)
    for h in range(4):
        qk = acc[:, h * 128 : h * 128 + 128].astype(bf16).astype(f32)
        sq = qk * qk
        s_lo = jnp.sum(jnp.where(lo, sq, 0.0), axis=1, keepdims=True)
        s_hi = jnp.sum(jnp.where(lo, 0.0, sq), axis=1, keepdims=True)
        inv = lax.rsqrt(jnp.where(lo, s_lo, s_hi) * (1 / 64) + 1e-6)
        out[h][at : at + 320, :] = (qk * inv * gains).astype(bf16)
        c = 512 + (h // 2) * 128
        top, bot = acc[:160, c : c + 128], acc[160:, c : c + 128]
        if h % 2:
            top = pltpu.roll(top, 64, 1)
        else:
            bot = pltpu.roll(bot, 64, 1)
        out[h][at + 320 : at + 480, :] = jnp.where(half, top, bot).astype(bf16)


def gain_row(gain_ref):
    return jnp.concatenate([gain_ref[0:1, :] * 0.125, gain_ref[1:2, :]], 1)


def proj_kernel(idx_ref, gain_ref, *refs, sizes):
    n = sum(sizes)
    toks, ws, outs, w = refs[:n], refs[n : n + 8], refs[n + 8 : n + 12], refs[-1]
    for j in range(8):
        cols = pl.ds(pl.multiple_of(idx_ref[j] * 256, 256), 256)
        for h in range(4):
            w[h * 128 : h * 128 + 128, cols] = ws[j][h * 192 : h * 192 + 128, :]
            w[512 + h * 64 : 576 + h * 64, cols] = ws[j][h * 192 + 128 : h * 192 + 192, :]
    gains = gain_row(gain_ref)
    at = 0
    for b, size in enumerate(sizes):
        parts = [t[...] for t in toks[at : at + size]]
        at += size
        tok = parts[0] if size == 1 else jnp.concatenate(parts, 0)
        proj_block(tok, w[...], gains, outs, b * 480)


def project(cols, gain, blocks, ws):
    toks = [p for block in blocks for p in block]
    return pl.pallas_call(
        functools.partial(proj_kernel, sizes=tuple(len(b) for b in blocks)),
        out_shape=[jax.ShapeDtypeStruct((len(blocks) * 480, 128), bf16)] * 4,
        in_specs=[SMEM] + [VMEM] * (1 + len(toks) + 8),
        out_specs=[VMEM] * 4,
        scratch_shapes=[pltpu.VMEM((768, 2048), bf16)],
        compiler_params=pltpu.CompilerParams(vmem_limit_bytes=20 * 1024 * 1024),
        name="project",
    )(cols, gain, *toks, *ws)


def out_kernel(head_ref, col_ref, heads_ref, *refs):
    ws, o_ref, lhs = refs[:8], refs[8], refs[9]
    half = lax.broadcasted_iota(jnp.int32, (BLK // 2, 128), 1) < 64
    for p in range(8):
        a = heads_ref[head_ref[2 * p]].astype(f32)
        b = heads_ref[head_ref[2 * p + 1]].astype(f32)
        s = slice(p * 128, p * 128 + 128)
        lhs[0:160, s] = jnp.where(half, a, pltpu.roll(b, 64, 1)).astype(bf16)
        lhs[160:320, s] = jnp.where(half, pltpu.roll(a, 64, 1), b).astype(bf16)
    for par in range(2):
        for dx in range(4):
            acc = None
            for dy in range(4):
                rhs = ws[par * 4 + dy][dx * 256 : dx * 256 + 256, :]
                part = lax.dot_general(
                    lhs[:, dy * 256 : dy * 256 + 256], rhs, NN, preferred_element_type=f32
                )
                acc = part if acc is None else acc + part
            cols = pl.ds(pl.multiple_of(col_ref[par * 4 + dx] * 256, 256), 256)
            o_ref[:, cols] = acc.astype(bf16)


def output(order, cols, heads, ws):
    return pl.pallas_call(
        out_kernel,
        out_shape=jax.ShapeDtypeStruct((BLK, 2048), bf16),
        in_specs=[SMEM, SMEM] + [VMEM] * 9,
        out_specs=VMEM,
        scratch_shapes=[pltpu.VMEM((BLK, 1024), bf16)],
        compiler_params=pltpu.CompilerParams(vmem_limit_bytes=12 * 1024 * 1024),
        name="output",
    )(order, cols, heads, *ws)


def turn(step):
    return [(i, (i + step) % 4) for i in range(4)]


def move(value, axis, step):
    pairs = [(0, 1), (1, 0)] if axis == C else turn(step)
    return lax.ppermute(value, axis, pairs)


def spread(value, step):
    pairs = [(2 * i + k, 2 * ((i + (step, -step)[k]) % 4) + k) for i in range(4) for k in (0, 1)]
    return lax.ppermute(value, (Y, C), pairs)


def around(value, axis):
    return [value] + [move(value, axis, -d) for d in (1, 2, 3)]


def on_device(tokens, w_query, w_key, w_value, w_output, qk_gain, decay_sums):
    own = tokens[0]
    z, y, x, c = (lax.axis_index(a) for a in (Z, Y, X, C))
    t1 = spread(own, -1)
    t3 = spread(own, 1)
    t2 = spread(t1, -1)
    near = jnp.where(c == 0, 1, 3)
    piece = jnp.concatenate([w_query.T, w_key.T, w_value.T, w_output], 0)
    w4, wo4 = pack(around(piece, Z))
    ws = around(w4, X)
    ws = ws + [move(w, C, 0) for w in ws]

    cols = jnp.stack(
        [2 * ((x + d) % 4) + e for e in (c, 1 - c) for d in range(4)]
    ).astype(jnp.int32)
    gain, decay = lax.optimization_barrier((qk_gain, decay_sums.reshape(8, 640)))
    part1 = project(cols, gain, [[own], [t1], [t3]], ws)
    *part1, wo4 = lax.optimization_barrier((*part1, wo4))
    part2 = project(cols, gain, [[t2]], ws)
    recv = []
    for part in (part1, part2):
        recv += [part[0]] + [move(part[d], Z, d) for d in (1, 2, 3)]
    wo16 = join(around(wo4, X))
    wo = around(wo16, Y)
    pos = [4 * ((z - d) % 4) + (y + e) % 4 for d in range(4) for e in (0, near, 4 - near)]
    pos += [4 * ((z - d) % 4) + (y + 2) % 4 for d in range(4)]
    pos = jnp.stack(pos).astype(jnp.int32)
    heads = attention(pos, gain, decay, recv, (3, 3, 3, 3, 1, 1, 1, 1))
    heads, *wo = lax.optimization_barrier((heads, *wo))
    wo = wo + [move(w, C, 0) for w in wo]
    merged = lax.all_to_all(heads, SP, 0, 0, tiled=True)
    order = jnp.stack(
        [4 * ((z + d) % 4) + (y + e) % 4 for e in range(4) for d in range(4)]
    ).astype(jnp.int32)
    return output(order, cols, merged, wo)[None]


def solution(mesh):
    torus = Mesh(mesh.devices.reshape(4, 4, 4, 2), ("sp_0", "sp_1", "dp_0", "dp_1"))
    in_specs = (P(DP, SP, None), P(DP, SP), P(DP, SP), P(DP, SP), P(SP, DP), P(), P(DP, SP, None))
    out_specs = P(DP, SP, None)
    return jax.shard_map(
        on_device, mesh=torus, in_specs=in_specs, out_specs=out_specs, check_vma=False
    )
```

```python
import functools

import jax
import jax.numpy as jnp
from jax import lax
from jax.experimental import pallas as pl
from jax.experimental.pallas import tpu as pltpu
from jax.sharding import Mesh
from jax.sharding import PartitionSpec as P


DP = ("dp_0", "dp_1")
SP = ("sp_0", "sp_1")
Z, Y, X, C = "sp_0", "sp_1", "dp_0", "dp_1"
LOG2E = 1.4426950408889634
T = 5120
BLK = 320
BQ = 512
W = 1024
NT = (((1,), (1,)), ((), ()))
NN = (((1,), (0,)), ((), ()))
f32 = jnp.float32
bf16 = jnp.bfloat16
SMEM = pl.BlockSpec(memory_space=pltpu.SMEM)
VMEM = pl.BlockSpec(memory_space=pltpu.VMEM)
HBM = pl.BlockSpec(memory_space=pltpu.HBM)


def attn_kernel(pos_ref, gain_ref, d_ref, *refs, nblk):
    nin=len(nblk)
    ins=refs[:nin]; out_ref=refs[nin]; ka,qa,vs,vt,ot=refs[nin+1:]
    lane=lax.broadcasted_iota(jnp.int32,(BLK,128),1)
    lo=lane<64
    lanev=lax.broadcasted_iota(jnp.int32,(BLK//2,128),1)
    tail=jnp.where(lanev==64,1.0,0.0)
    n=0
    for a,nb in zip(ins,nblk):
        for b in range(nb):
            base=pl.multiple_of(pos_ref[n]*BLK,64); n+=1
            qk=a[b*480:b*480+320,:].astype(f32)
            rolled=pltpu.roll(qk,64,1)
            ka[pl.ds(base,BLK),0:128]=jnp.where(lo,rolled,qk).astype(bf16)
            qs=jnp.where(lo,qk,rolled)*LOG2E
            hi=qs.astype(bf16).astype(f32)
            qa[pl.ds(base,BLK),0:128]=jnp.where(lo,hi,qs-hi).astype(bf16)
            v=a[b*480+320:b*480+480,:].astype(f32)
            vs[pl.ds(base,BLK//2),:]=jnp.where(lanev<64,v,tail)
            vs[pl.ds(base+BLK//2,BLK//2),:]=jnp.where(lanev<64,pltpu.roll(v,64,1),tail)
    x=jnp.concatenate([d_ref[0:1,i*640:(i+1)*640] for i in range(8)],0)*LOG2E
    h=x.astype(bf16).astype(f32)
    m=(x-h).astype(bf16).astype(f32)
    l=x-h-m
    dt=jnp.concatenate([-h,-m,-l,h,m,l,jnp.zeros((80,640),f32)],0).T
    dl=lax.broadcasted_iota(jnp.int32,(640,128),1)
    key_one=jnp.where((dl>=24)&(dl<48),1.0,0.0)
    query_one=jnp.where(dl<24,1.0,0.0)
    for i in range(T//640):
        s=slice(i*640,(i+1)*640)
        ka[s,128:256]=jnp.where((dl==i)|(dl==8+i)|(dl==16+i),dt,key_one).astype(bf16)
        qa[s,128:256]=jnp.where((dl==24+i)|(dl==32+i)|(dl==40+i),dt,query_one).astype(bf16)
    for i in range(T//256):
        vt[:,i*256:(i+1)*256]=vs[i*256:(i+1)*256,:].T[0:80].astype(bf16)

    def finish(acc):
        o=acc[0:64]/acc[64:65]
        return o*lax.rsqrt(jnp.mean(o*o,axis=0,keepdims=True)+1e-6)

    def fast():
        kio=lax.broadcasted_iota(jnp.int32,(BQ,BQ),0); qio=lax.broadcasted_iota(jnp.int32,(BQ,BQ),1)
        keep=kio<=qio
        for qi in range(T//BQ):
            q0=qi*BQ
            qb=qa[q0:q0+BQ,:]
            def tile(k0,w,mask):
                s=lax.dot_general(ka[k0:k0+w,:],qb,NT,preferred_element_type=f32)
                p=jnp.exp2(s)
                if mask:
                    p=jnp.where(keep,p,0.0)
                return lax.dot_general(vt[:,k0:k0+w],p.astype(bf16),NN,preferred_element_type=f32)
            acc=tile(q0,BQ,True)
            for k0 in range(0,q0,W):
                acc=acc+tile(k0,min(W,q0-k0),False)
            ot[:,q0:q0+BQ]=finish(acc)

    def slow():
        kio=lax.broadcasted_iota(jnp.int32,(BQ,BQ),0); qio=lax.broadcasted_iota(jnp.int32,(BQ,BQ),1)
        def per_q(qi,_):
            q0=pl.multiple_of(qi*BQ,BQ)
            qb=qa[pl.ds(q0,BQ),:]
            def body(j,c):
                m,acc=c
                k0=pl.multiple_of(j*BQ,BQ)
                s=lax.dot_general(ka[pl.ds(k0,BQ),:],qb,NT,preferred_element_type=f32)
                s=jnp.where(kio+k0<=qio+q0,s,-jnp.inf)
                m2=jnp.maximum(m,jnp.max(s,axis=0,keepdims=True))
                p=jnp.exp2(s-m2).astype(bf16)
                acc=acc*jnp.exp2(m-m2)+lax.dot_general(vt[:,pl.ds(k0,BQ)],p,NN,preferred_element_type=f32)
                return m2,acc
            m0=jnp.full((1,BQ),-jnp.inf,f32)
            c=body(qi,(m0,jnp.zeros((80,BQ),f32)))
            _,acc=lax.fori_loop(0,qi,body,c)
            ot[:,pl.ds(q0,BQ)]=finish(acc)
            return 0
        lax.fori_loop(0,T//BQ,per_q,0)
    g=jnp.abs(gain_ref[...])
    isfast=jnp.max(g[0:1])*jnp.max(g[1:2])<=7.7
    pl.when(isfast)(fast)
    pl.when(jnp.logical_not(isfast))(slow)
    for i in range(T//256):
        s=slice(i*256,(i+1)*256)
        vs[s,0:64]=ot[:,s].T
    for j in range(T//BLK):
        a=vs[j*BLK:j*BLK+160,:]; b=vs[j*BLK+160:(j+1)*BLK,:]
        out_ref[j]=jnp.where(lanev<64,a,pltpu.roll(b,64,1)).astype(bf16)


def attention(pos,gain,d,ins,nblk):
    V=pltpu.VMEM
    return pl.pallas_call(functools.partial(attn_kernel,nblk=nblk),
        out_shape=jax.ShapeDtypeStruct((16,160,128),bf16),
        in_specs=[SMEM]+[VMEM]*(2+len(ins)),
        out_specs=VMEM,
        scratch_shapes=[V((T,256),bf16),V((T,256),bf16),V((T,128),f32),V((80,T),bf16),V((64,T),f32)],
        compiler_params=pltpu.CompilerParams(vmem_limit_bytes=24*1024*1024),
        name="attention")(pos,gain,d,*ins)


def pack_kernel(*refs):
    ins, w, wo = refs[:4], refs[4], refs[5]
    for h in range(4):
        w[h * 192 : h * 192 + 192, :] = ins[h][0:192, :]
        wo[h * 64 : h * 64 + 64, :] = ins[h][192:256, :]


def pack(pieces):
    return pl.pallas_call(
        pack_kernel,
        out_shape=[jax.ShapeDtypeStruct((768, 256), bf16), jax.ShapeDtypeStruct((256, 256), bf16)],
        in_specs=[VMEM] * 4,
        out_specs=[VMEM] * 2,
        compiler_params=pltpu.CompilerParams(vmem_limit_bytes=4 * 1024 * 1024),
        name="pack",
    )(*pieces)


def join_kernel(*refs):
    for i in range(4):
        refs[4][i * 256 : i * 256 + 256, :] = refs[i][...]


def join(pieces):
    return pl.pallas_call(
        join_kernel,
        out_shape=jax.ShapeDtypeStruct((1024, 256), bf16),
        in_specs=[VMEM] * 4,
        out_specs=VMEM,
        compiler_params=pltpu.CompilerParams(vmem_limit_bytes=4 * 1024 * 1024),
        name="join",
    )(*pieces)


def proj_block(tok, w, gains, out, at):
    lo = lax.broadcasted_iota(jnp.int32, (BLK, 128), 1) < 64
    half = lax.broadcasted_iota(jnp.int32, (BLK // 2, 128), 1) < 64
    acc = lax.dot_general(tok, w, NT, preferred_element_type=f32)
    for h in range(4):
        qk = acc[:, h * 128 : h * 128 + 128].astype(bf16).astype(f32)
        sq = qk * qk
        s_lo = jnp.sum(jnp.where(lo, sq, 0.0), axis=1, keepdims=True)
        s_hi = jnp.sum(jnp.where(lo, 0.0, sq), axis=1, keepdims=True)
        inv = lax.rsqrt(jnp.where(lo, s_lo, s_hi) * (1 / 64) + 1e-6)
        out[h][at : at + 320, :] = (qk * inv * gains).astype(bf16)
        c = 512 + (h // 2) * 128
        top, bot = acc[:160, c : c + 128], acc[160:, c : c + 128]
        if h % 2:
            top = pltpu.roll(top, 64, 1)
        else:
            bot = pltpu.roll(bot, 64, 1)
        out[h][at + 320 : at + 480, :] = jnp.where(half, top, bot).astype(bf16)


def gain_row(gain_ref):
    return jnp.concatenate([gain_ref[0:1, :] * 0.125, gain_ref[1:2, :]], 1)


def proj_kernel(idx_ref, gain_ref, *refs, count):
    toks, ws, outs = refs[:count], refs[count : count + 8], refs[count + 8 : count + 12]
    tv, wv, w, sem_t, sem_w = refs[count + 12 :]
    loads = [pltpu.make_async_copy(ws[j], wv.at[j], sem_w.at[j]) for j in range(8)]
    fetch = [pltpu.make_async_copy(toks[b], tv.at[b], sem_t.at[b]) for b in range(count)]
    for copy in loads + fetch:
        copy.start()
    for j in range(8):
        loads[j].wait()
        cols = pl.ds(pl.multiple_of(idx_ref[j] * 256, 256), 256)
        for h in range(4):
            w[h * 128 : h * 128 + 128, cols] = wv[j, h * 192 : h * 192 + 128, :]
            w[512 + h * 64 : 576 + h * 64, cols] = wv[j, h * 192 + 128 : h * 192 + 192, :]
    gains = gain_row(gain_ref)
    for b in range(count):
        fetch[b].wait()
        proj_block(tv[b], w[...], gains, outs, b * 480)


def project(cols, gain, toks, ws):
    count = len(toks)
    return pl.pallas_call(
        functools.partial(proj_kernel, count=count),
        out_shape=[jax.ShapeDtypeStruct((count * 480, 128), bf16)] * 4,
        in_specs=[SMEM, VMEM] + [HBM] * (count + 8),
        out_specs=[VMEM] * 4,
        scratch_shapes=[
            pltpu.VMEM((count, BLK, 2048), bf16),
            pltpu.VMEM((8, 768, 256), bf16),
            pltpu.VMEM((768, 2048), bf16),
            pltpu.SemaphoreType.DMA((count,)),
            pltpu.SemaphoreType.DMA((8,)),
        ],
        compiler_params=pltpu.CompilerParams(vmem_limit_bytes=24 * 1024 * 1024),
        name="project",
    )(cols, gain, *toks, *ws)


def out_kernel(head_ref, col_ref, heads_ref, *refs):
    ws, o_ref, lhs = refs[:8], refs[8], refs[9]
    half = lax.broadcasted_iota(jnp.int32, (BLK // 2, 128), 1) < 64
    for p in range(8):
        a = heads_ref[head_ref[2 * p]].astype(f32)
        b = heads_ref[head_ref[2 * p + 1]].astype(f32)
        s = slice(p * 128, p * 128 + 128)
        lhs[0:160, s] = jnp.where(half, a, pltpu.roll(b, 64, 1)).astype(bf16)
        lhs[160:320, s] = jnp.where(half, pltpu.roll(a, 64, 1), b).astype(bf16)
    for par in range(2):
        for dx in range(4):
            acc = None
            for dy in range(4):
                rhs = ws[par * 4 + dy][dx * 256 : dx * 256 + 256, :]
                part = lax.dot_general(
                    lhs[:, dy * 256 : dy * 256 + 256], rhs, NN, preferred_element_type=f32
                )
                acc = part if acc is None else acc + part
            cols = pl.ds(pl.multiple_of(col_ref[par * 4 + dx] * 256, 256), 256)
            o_ref[:, cols] = acc.astype(bf16)


def output(order, cols, heads, ws):
    return pl.pallas_call(
        out_kernel,
        out_shape=jax.ShapeDtypeStruct((BLK, 2048), bf16),
        in_specs=[SMEM, SMEM] + [VMEM] * 9,
        out_specs=VMEM,
        scratch_shapes=[pltpu.VMEM((BLK, 1024), bf16)],
        compiler_params=pltpu.CompilerParams(vmem_limit_bytes=12 * 1024 * 1024),
        name="output",
    )(order, cols, heads, *ws)


def turn(step):
    return [(i, (i + step) % 4) for i in range(4)]


def move(value, axis, step):
    pairs = [(0, 1), (1, 0)] if axis == C else turn(step)
    return lax.ppermute(value, axis, pairs)


def spread(value, step):
    pairs = [(2 * i + k, 2 * ((i + (step, -step)[k]) % 4) + k) for i in range(4) for k in (0, 1)]
    return lax.ppermute(value, (Y, C), pairs)


def around(value, axis):
    return [value] + [move(value, axis, -d) for d in (1, 2, 3)]


def on_device(tokens, w_query, w_key, w_value, w_output, qk_gain, decay_sums):
    own = tokens[0]
    z, y, x, c = (lax.axis_index(a) for a in (Z, Y, X, C))
    t1 = spread(own, -1)
    t3 = spread(own, 1)
    t2 = spread(t1, -1)
    near = jnp.where(c == 0, 1, 3)
    piece = jnp.concatenate([w_query.T, w_key.T, w_value.T, w_output], 0)
    w4, wo4 = pack(around(piece, Z))
    ws = around(w4, X)
    ws = ws + [move(w, C, 0) for w in ws]

    cols = jnp.stack(
        [2 * ((x + d) % 4) + e for e in (c, 1 - c) for d in range(4)]
    ).astype(jnp.int32)
    part1 = project(cols, qk_gain, [own, t1, t3], ws)
    *part1, wo4 = lax.optimization_barrier((*part1, wo4))
    part2 = project(cols, qk_gain, [t2], ws)
    recv = []
    for part in (part1, part2):
        recv += [part[0]] + [move(part[d], Z, d) for d in (1, 2, 3)]
    wo16 = join(around(wo4, X))
    wo = around(wo16, Y)
    pos = [4 * ((z - d) % 4) + (y + e) % 4 for d in range(4) for e in (0, near, 4 - near)]
    pos += [4 * ((z - d) % 4) + (y + 2) % 4 for d in range(4)]
    pos = jnp.stack(pos).astype(jnp.int32)
    heads = attention(pos, qk_gain, decay_sums[0], recv, (3, 3, 3, 3, 1, 1, 1, 1))
    heads, *wo = lax.optimization_barrier((heads, *wo))
    wo = wo + [move(w, C, 0) for w in wo]
    merged = lax.all_to_all(heads, SP, 0, 0, tiled=True)
    order = jnp.stack(
        [4 * ((z + d) % 4) + (y + e) % 4 for e in range(4) for d in range(4)]
    ).astype(jnp.int32)
    return output(order, cols, merged, wo)[None]


def solution(mesh):
    torus = Mesh(mesh.devices.reshape(4, 4, 4, 2), ("sp_0", "sp_1", "dp_0", "dp_1"))
    in_specs = (P(DP, SP, None), P(DP, SP), P(DP, SP), P(DP, SP), P(SP, DP), P(), P(DP, SP, None))
    out_specs = P(DP, SP, None)
    return jax.shard_map(
        on_device, mesh=torus, in_specs=in_specs, out_specs=out_specs, check_vma=False
    )
```

```python
import functools

import jax
import jax.numpy as jnp
from jax import lax
from jax.experimental import pallas as pl
from jax.experimental.pallas import tpu as pltpu
from jax.sharding import Mesh
from jax.sharding import PartitionSpec as P


DP = ("dp_0", "dp_1")
SP = ("sp_0", "sp_1")
Z, Y, X, C = "sp_0", "sp_1", "dp_0", "dp_1"
LOG2E = 1.4426950408889634
T = 5120
BLK = 320
BQ = 512
W = 2048
NT = (((1,), (1,)), ((), ()))
NN = (((1,), (0,)), ((), ()))
f32 = jnp.float32
bf16 = jnp.bfloat16
SMEM = pl.BlockSpec(memory_space=pltpu.SMEM)
VMEM = pl.BlockSpec(memory_space=pltpu.VMEM)


def attn_kernel(pos_ref, gain_ref, d_ref, *refs, nblk):
    nin=len(nblk)
    ins=refs[:nin]; out_ref=refs[nin]; ka,qa,vs,vt,ot,rows=refs[nin+1:]
    lane=lax.broadcasted_iota(jnp.int32,(BLK,128),1)
    lo=lane<64
    lanev=lax.broadcasted_iota(jnp.int32,(BLK//2,128),1)
    tail=jnp.where(lanev==64,1.0,0.0)
    n=0
    for a,nb in zip(ins,nblk):
        for b in range(nb):
            base=pl.multiple_of(pos_ref[n]*BLK,64); n+=1
            qk=a[b*480:b*480+320,:].astype(f32)
            rolled=pltpu.roll(qk,64,1)
            ka[pl.ds(base,BLK),0:128]=jnp.where(lo,rolled,qk).astype(bf16)
            qs=jnp.where(lo,qk,rolled)*LOG2E
            hi=qs.astype(bf16).astype(f32)
            qa[pl.ds(base,BLK),0:128]=jnp.where(lo,hi,qs-hi).astype(bf16)
            v=a[b*480+320:b*480+480,:].astype(f32)
            vs[pl.ds(base,BLK//2),:]=jnp.where(lanev<64,v,tail)
            vs[pl.ds(base+BLK//2,BLK//2),:]=jnp.where(lanev<64,pltpu.roll(v,64,1),tail)
    x=jnp.concatenate([d_ref[0:1,i*BQ:(i+1)*BQ] for i in range(T//BQ)]+[jnp.zeros((16-T//BQ,BQ),f32)],0)*LOG2E
    h=x.astype(bf16).astype(f32)
    m=(x-h).astype(bf16).astype(f32)
    l=x-h-m
    dt=jnp.concatenate([-h,-m,-l,h,m,l,jnp.zeros((32,BQ),f32)],0).T
    dl=lax.broadcasted_iota(jnp.int32,(BQ,128),1)
    key_one=jnp.where((dl>=48)&(dl<96),1.0,0.0)
    query_one=jnp.where(dl<48,1.0,0.0)

    def prepare(i):
        s=slice(i*BQ,(i+1)*BQ)
        ka[s,128:256]=jnp.where((dl==i)|(dl==16+i)|(dl==32+i),dt,key_one).astype(bf16)
        qa[s,128:256]=jnp.where((dl==48+i)|(dl==64+i)|(dl==80+i),dt,query_one).astype(bf16)
        vt[:,s]=vs[s,:].T[0:80].astype(bf16)

    def emit(i):
        s=slice(i*BQ,(i+1)*BQ)
        rows[s,0:64]=ot[:,s].T
        for j in range(T//BLK):
            if i*BQ<(j+1)*BLK<=(i+1)*BQ:
                a=rows[j*BLK:j*BLK+160,:]
                b=rows[j*BLK+160:(j+1)*BLK,:]
                out_ref[j]=jnp.where(lanev<64,a,pltpu.roll(b,64,1)).astype(bf16)

    def finish(acc):
        o=acc[0:64]/acc[64:65]
        return o*lax.rsqrt(jnp.mean(o*o,axis=0,keepdims=True)+1e-6)

    def fast():
        kio=lax.broadcasted_iota(jnp.int32,(BQ,BQ),0); qio=lax.broadcasted_iota(jnp.int32,(BQ,BQ),1)
        keep=kio<=qio
        for qi in range(T//BQ):
            q0=qi*BQ
            prepare(qi)
            qb=qa[q0:q0+BQ,:]
            def tile(k0,w,mask):
                s=lax.dot_general(ka[k0:k0+w,:],qb,NT,preferred_element_type=f32)
                p=jnp.exp2(s)
                if mask:
                    p=jnp.where(keep,p,0.0)
                return lax.dot_general(vt[:,k0:k0+w],p.astype(bf16),NN,preferred_element_type=f32)
            acc=tile(q0,BQ,True)
            for k0 in range(0,q0,W):
                acc=acc+tile(k0,min(W,q0-k0),False)
            ot[:,q0:q0+BQ]=finish(acc)
            emit(qi)

    def slow():
        for i in range(T//BQ):
            prepare(i)
        kio=lax.broadcasted_iota(jnp.int32,(BQ,BQ),0); qio=lax.broadcasted_iota(jnp.int32,(BQ,BQ),1)
        def per_q(qi,_):
            q0=pl.multiple_of(qi*BQ,BQ)
            qb=qa[pl.ds(q0,BQ),:]
            def body(j,c):
                m,acc=c
                k0=pl.multiple_of(j*BQ,BQ)
                s=lax.dot_general(ka[pl.ds(k0,BQ),:],qb,NT,preferred_element_type=f32)
                s=jnp.where(kio+k0<=qio+q0,s,-jnp.inf)
                m2=jnp.maximum(m,jnp.max(s,axis=0,keepdims=True))
                p=jnp.exp2(s-m2).astype(bf16)
                acc=acc*jnp.exp2(m-m2)+lax.dot_general(vt[:,pl.ds(k0,BQ)],p,NN,preferred_element_type=f32)
                return m2,acc
            m0=jnp.full((1,BQ),-jnp.inf,f32)
            c=body(qi,(m0,jnp.zeros((80,BQ),f32)))
            _,acc=lax.fori_loop(0,qi,body,c)
            ot[:,pl.ds(q0,BQ)]=finish(acc)
            return 0
        lax.fori_loop(0,T//BQ,per_q,0)
        for i in range(T//BQ):
            emit(i)
    g=jnp.abs(gain_ref[...])
    isfast=jnp.max(g[0:1])*jnp.max(g[1:2])<=7.7
    pl.when(isfast)(fast)
    pl.when(jnp.logical_not(isfast))(slow)


def attention(pos,gain,d,ins,nblk):
    V=pltpu.VMEM
    return pl.pallas_call(functools.partial(attn_kernel,nblk=nblk),
        out_shape=jax.ShapeDtypeStruct((16,160,128),bf16),
        in_specs=[SMEM]+[VMEM]*(2+len(ins)),
        out_specs=VMEM,
        scratch_shapes=[V((T,256),bf16),V((T,256),bf16),V((T,128),f32),V((80,T),bf16),V((64,T),f32),V((T,128),f32)],
        compiler_params=pltpu.CompilerParams(vmem_limit_bytes=24*1024*1024),
        name="attention")(pos,gain,d,*ins)


def pack_kernel(*refs):
    ins, w, wo = refs[:4], refs[4], refs[5]
    for h in range(4):
        w[h * 192 : h * 192 + 192, :] = ins[h][0:192, :]
        wo[h * 64 : h * 64 + 64, :] = ins[h][192:256, :]


def pack(pieces):
    return pl.pallas_call(
        pack_kernel,
        out_shape=[jax.ShapeDtypeStruct((768, 256), bf16), jax.ShapeDtypeStruct((256, 256), bf16)],
        in_specs=[VMEM] * 4,
        out_specs=[VMEM] * 2,
        compiler_params=pltpu.CompilerParams(vmem_limit_bytes=4 * 1024 * 1024),
        name="pack",
    )(*pieces)


def join_kernel(*refs):
    for i in range(4):
        refs[4][i * 256 : i * 256 + 256, :] = refs[i][...]


def join(pieces):
    return pl.pallas_call(
        join_kernel,
        out_shape=jax.ShapeDtypeStruct((1024, 256), bf16),
        in_specs=[VMEM] * 4,
        out_specs=VMEM,
        compiler_params=pltpu.CompilerParams(vmem_limit_bytes=4 * 1024 * 1024),
        name="join",
    )(*pieces)


def proj_block(tok, w, gains, out, at):
    lo = lax.broadcasted_iota(jnp.int32, (BLK, 128), 1) < 64
    half = lax.broadcasted_iota(jnp.int32, (BLK // 2, 128), 1) < 64
    acc = lax.dot_general(tok, w, NT, preferred_element_type=f32)
    for h in range(4):
        qk = acc[:, h * 128 : h * 128 + 128].astype(bf16).astype(f32)
        sq = qk * qk
        s_lo = jnp.sum(jnp.where(lo, sq, 0.0), axis=1, keepdims=True)
        s_hi = jnp.sum(jnp.where(lo, 0.0, sq), axis=1, keepdims=True)
        inv = lax.rsqrt(jnp.where(lo, s_lo, s_hi) * (1 / 64) + 1e-6)
        out[h][at : at + 320, :] = (qk * inv * gains).astype(bf16)
        c = 512 + (h // 2) * 128
        top, bot = acc[:160, c : c + 128], acc[160:, c : c + 128]
        if h % 2:
            top = pltpu.roll(top, 64, 1)
        else:
            bot = pltpu.roll(bot, 64, 1)
        out[h][at + 320 : at + 480, :] = jnp.where(half, top, bot).astype(bf16)


def gain_row(gain_ref):
    return jnp.concatenate([gain_ref[0:1, :] * 0.125, gain_ref[1:2, :]], 1)


def proj_kernel(idx_ref, gain_ref, *refs, sizes):
    n = sum(sizes)
    toks, ws, outs, w = refs[:n], refs[n : n + 8], refs[n + 8 : n + 12], refs[-1]
    for j in range(8):
        cols = pl.ds(pl.multiple_of(idx_ref[j] * 256, 256), 256)
        for h in range(4):
            w[h * 128 : h * 128 + 128, cols] = ws[j][h * 192 : h * 192 + 128, :]
            w[512 + h * 64 : 576 + h * 64, cols] = ws[j][h * 192 + 128 : h * 192 + 192, :]
    gains = gain_row(gain_ref)
    at = 0
    for b, size in enumerate(sizes):
        parts = [t[...] for t in toks[at : at + size]]
        at += size
        tok = parts[0] if size == 1 else jnp.concatenate(parts, 0)
        proj_block(tok, w[...], gains, outs, b * 480)


def project(cols, gain, blocks, ws):
    toks = [p for block in blocks for p in block]
    return pl.pallas_call(
        functools.partial(proj_kernel, sizes=tuple(len(b) for b in blocks)),
        out_shape=[jax.ShapeDtypeStruct((len(blocks) * 480, 128), bf16)] * 4,
        in_specs=[SMEM] + [VMEM] * (1 + len(toks) + 8),
        out_specs=[VMEM] * 4,
        scratch_shapes=[pltpu.VMEM((768, 2048), bf16)],
        compiler_params=pltpu.CompilerParams(vmem_limit_bytes=20 * 1024 * 1024),
        name="project",
    )(cols, gain, *toks, *ws)


def out_kernel(head_ref, col_ref, heads_ref, *refs):
    ws, o_ref, lhs = refs[:8], refs[8], refs[9]
    half = lax.broadcasted_iota(jnp.int32, (BLK // 2, 128), 1) < 64
    for p in range(8):
        a = heads_ref[head_ref[2 * p]].astype(f32)
        b = heads_ref[head_ref[2 * p + 1]].astype(f32)
        s = slice(p * 128, p * 128 + 128)
        lhs[0:160, s] = jnp.where(half, a, pltpu.roll(b, 64, 1)).astype(bf16)
        lhs[160:320, s] = jnp.where(half, pltpu.roll(a, 64, 1), b).astype(bf16)
    for par in range(2):
        for dx in range(4):
            acc = None
            for dy in range(4):
                rhs = ws[par * 4 + dy][dx * 256 : dx * 256 + 256, :]
                part = lax.dot_general(
                    lhs[:, dy * 256 : dy * 256 + 256], rhs, NN, preferred_element_type=f32
                )
                acc = part if acc is None else acc + part
            cols = pl.ds(pl.multiple_of(col_ref[par * 4 + dx] * 256, 256), 256)
            o_ref[:, cols] = acc.astype(bf16)


def output(order, cols, heads, ws):
    return pl.pallas_call(
        out_kernel,
        out_shape=jax.ShapeDtypeStruct((BLK, 2048), bf16),
        in_specs=[SMEM, SMEM] + [VMEM] * 9,
        out_specs=VMEM,
        scratch_shapes=[pltpu.VMEM((BLK, 1024), bf16)],
        compiler_params=pltpu.CompilerParams(vmem_limit_bytes=12 * 1024 * 1024),
        name="output",
    )(order, cols, heads, *ws)


def turn(step):
    return [(i, (i + step) % 4) for i in range(4)]


def move(value, axis, step):
    pairs = [(0, 1), (1, 0)] if axis == C else turn(step)
    return lax.ppermute(value, axis, pairs)


def spread(value, step):
    pairs = [(2 * i + k, 2 * ((i + (step, -step)[k]) % 4) + k) for i in range(4) for k in (0, 1)]
    return lax.ppermute(value, (Y, C), pairs)


def around(value, axis):
    return [value] + [move(value, axis, -d) for d in (1, 2, 3)]


def on_device(tokens, w_query, w_key, w_value, w_output, qk_gain, decay_sums):
    own = tokens[0]
    z, y, x, c = (lax.axis_index(a) for a in (Z, Y, X, C))
    t1 = spread(own, -1)
    t3 = spread(own, 1)
    t2 = spread(t1, -1)
    near = jnp.where(c == 0, 1, 3)
    piece = jnp.concatenate([w_query.T, w_key.T, w_value.T, w_output], 0)
    w4, wo4 = pack(around(piece, Z))
    ws = around(w4, X)
    ws = ws + [move(w, C, 0) for w in ws]

    cols = jnp.stack(
        [2 * ((x + d) % 4) + e for e in (c, 1 - c) for d in range(4)]
    ).astype(jnp.int32)
    part1 = project(cols, qk_gain, [[own], [t1], [t3]], ws)
    *part1, wo4 = lax.optimization_barrier((*part1, wo4))
    part2 = project(cols, qk_gain, [[t2]], ws)
    recv = []
    for part in (part1, part2):
        recv += [part[0]] + [move(part[d], Z, d) for d in (1, 2, 3)]
    wo16 = join(around(wo4, X))
    wo = around(wo16, Y)
    pos = [4 * ((z - d) % 4) + (y + e) % 4 for d in range(4) for e in (0, near, 4 - near)]
    pos += [4 * ((z - d) % 4) + (y + 2) % 4 for d in range(4)]
    pos = jnp.stack(pos).astype(jnp.int32)
    heads = attention(pos, qk_gain, decay_sums[0], recv, (3, 3, 3, 3, 1, 1, 1, 1))
    heads, *wo = lax.optimization_barrier((heads, *wo))
    wo = wo + [move(w, C, 0) for w in wo]
    merged = lax.all_to_all(heads, SP, 0, 0, tiled=True)
    order = jnp.stack(
        [4 * ((z + d) % 4) + (y + e) % 4 for e in range(4) for d in range(4)]
    ).astype(jnp.int32)
    return output(order, cols, merged, wo)[None]


def solution(mesh):
    torus = Mesh(mesh.devices.reshape(4, 4, 4, 2), ("sp_0", "sp_1", "dp_0", "dp_1"))
    in_specs = (P(DP, SP, None), P(DP, SP), P(DP, SP), P(DP, SP), P(SP, DP), P(), P(DP, SP, None))
    out_specs = P(DP, SP, None)
    return jax.shard_map(
        on_device, mesh=torus, in_specs=in_specs, out_specs=out_specs, check_vma=False
    )
```

```python
import functools

import jax
import jax.numpy as jnp
from jax import lax
from jax.experimental import pallas as pl
from jax.experimental.pallas import tpu as pltpu
from jax.sharding import Mesh
from jax.sharding import PartitionSpec as P


DP = ("dp_0", "dp_1")
SP = ("sp_0", "sp_1")
Z, Y, X, C = "sp_0", "sp_1", "dp_0", "dp_1"
LOG2E = 1.4426950408889634
T = 5120
BLK = 320
BQ = 512
W = 2048
NT = (((1,), (1,)), ((), ()))
NN = (((1,), (0,)), ((), ()))
f32 = jnp.float32
bf16 = jnp.bfloat16
SMEM = pl.BlockSpec(memory_space=pltpu.SMEM)
VMEM = pl.BlockSpec(memory_space=pltpu.VMEM)


def attn_kernel(pos_ref, gain_ref, d_ref, *refs, nblk):
    nin=len(nblk)
    ins=refs[:nin]; out_ref=refs[nin]; ka,qa,vs,vt,ot,rows=refs[nin+1:]
    lane=lax.broadcasted_iota(jnp.int32,(BLK,128),1)
    lo=lane<64
    lanev=lax.broadcasted_iota(jnp.int32,(BLK//2,128),1)
    tail=jnp.where(lanev==64,1.0,0.0)
    n=0
    for a,nb in zip(ins,nblk):
        for b in range(nb):
            base=pl.multiple_of(pos_ref[n]*BLK,64); n+=1
            qk=a[b*480:b*480+320,:].astype(f32)
            rolled=pltpu.roll(qk,64,1)
            ka[pl.ds(base,BLK),0:128]=jnp.where(lo,rolled,qk).astype(bf16)
            qs=jnp.where(lo,qk,rolled)*LOG2E
            hi=qs.astype(bf16).astype(f32)
            qa[pl.ds(base,BLK),0:128]=jnp.where(lo,hi,qs-hi).astype(bf16)
            v=a[b*480+320:b*480+480,:].astype(f32)
            vs[pl.ds(base,BLK//2),:]=jnp.where(lanev<64,v,tail)
            vs[pl.ds(base+BLK//2,BLK//2),:]=jnp.where(lanev<64,pltpu.roll(v,64,1),tail)
    x=jnp.concatenate([d_ref[0:1,i*BQ:(i+1)*BQ] for i in range(T//BQ)]+[jnp.zeros((16-T//BQ,BQ),f32)],0)*LOG2E
    h=x.astype(bf16).astype(f32)
    m=(x-h).astype(bf16).astype(f32)
    l=x-h-m
    dt=jnp.concatenate([-h,-m,-l,h,m,l,jnp.zeros((32,BQ),f32)],0).T
    dl=lax.broadcasted_iota(jnp.int32,(BQ,128),1)
    key_one=jnp.where((dl>=48)&(dl<96),1.0,0.0)
    query_one=jnp.where(dl<48,1.0,0.0)

    def prepare(i):
        s=slice(i*BQ,(i+1)*BQ)
        ka[s,128:256]=jnp.where((dl==i)|(dl==16+i)|(dl==32+i),dt,key_one).astype(bf16)
        qa[s,128:256]=jnp.where((dl==48+i)|(dl==64+i)|(dl==80+i),dt,query_one).astype(bf16)
        vt[:,s]=vs[s,:].T[0:80].astype(bf16)

    def emit(i):
        s=slice(i*BQ,(i+1)*BQ)
        rows[s,0:64]=ot[:,s].T
        for j in range(T//BLK):
            if i*BQ<(j+1)*BLK<=(i+1)*BQ:
                a=rows[j*BLK:j*BLK+160,:]
                b=rows[j*BLK+160:(j+1)*BLK,:]
                out_ref[j]=jnp.where(lanev<64,a,pltpu.roll(b,64,1)).astype(bf16)

    def finish(acc):
        o=acc[0:64]/acc[64:65]
        return o*lax.rsqrt(jnp.mean(o*o,axis=0,keepdims=True)+1e-6)

    def fast():
        kio=lax.broadcasted_iota(jnp.int32,(BQ,BQ),0); qio=lax.broadcasted_iota(jnp.int32,(BQ,BQ),1)
        keep=kio<=qio
        for qi in range(T//BQ):
            q0=qi*BQ
            prepare(qi)
            qb=qa[q0:q0+BQ,:]
            def tile(k0,w,mask):
                s=lax.dot_general(ka[k0:k0+w,:],qb,NT,preferred_element_type=f32)
                p=jnp.exp2(s)
                if mask:
                    p=jnp.where(keep,p,0.0)
                return lax.dot_general(vt[:,k0:k0+w],p.astype(bf16),NN,preferred_element_type=f32)
            acc=tile(q0,BQ,True)
            for k0 in range(0,q0,W):
                acc=acc+tile(k0,min(W,q0-k0),False)
            ot[:,q0:q0+BQ]=finish(acc)
            emit(qi)

    def slow():
        for i in range(T//BQ):
            prepare(i)
        kio=lax.broadcasted_iota(jnp.int32,(BQ,BQ),0); qio=lax.broadcasted_iota(jnp.int32,(BQ,BQ),1)
        def per_q(qi,_):
            q0=pl.multiple_of(qi*BQ,BQ)
            qb=qa[pl.ds(q0,BQ),:]
            def body(j,c):
                m,acc=c
                k0=pl.multiple_of(j*BQ,BQ)
                s=lax.dot_general(ka[pl.ds(k0,BQ),:],qb,NT,preferred_element_type=f32)
                s=jnp.where(kio+k0<=qio+q0,s,-jnp.inf)
                m2=jnp.maximum(m,jnp.max(s,axis=0,keepdims=True))
                p=jnp.exp2(s-m2).astype(bf16)
                acc=acc*jnp.exp2(m-m2)+lax.dot_general(vt[:,pl.ds(k0,BQ)],p,NN,preferred_element_type=f32)
                return m2,acc
            m0=jnp.full((1,BQ),-jnp.inf,f32)
            c=body(qi,(m0,jnp.zeros((80,BQ),f32)))
            _,acc=lax.fori_loop(0,qi,body,c)
            ot[:,pl.ds(q0,BQ)]=finish(acc)
            return 0
        lax.fori_loop(0,T//BQ,per_q,0)
        for i in range(T//BQ):
            emit(i)
    g=jnp.abs(gain_ref[...])
    isfast=jnp.max(g[:,0:64])*jnp.max(g[:,64:128])<=7.7/8
    pl.when(isfast)(fast)
    pl.when(jnp.logical_not(isfast))(slow)


def attention(pos,gain,d,ins,nblk):
    V=pltpu.VMEM
    return pl.pallas_call(functools.partial(attn_kernel,nblk=nblk),
        out_shape=jax.ShapeDtypeStruct((16,160,128),bf16),
        in_specs=[SMEM]+[VMEM]*(2+len(ins)),
        out_specs=VMEM,
        scratch_shapes=[V((T,256),bf16),V((T,256),bf16),V((T,128),f32),V((80,T),bf16),V((64,T),f32),V((T,128),f32)],
        compiler_params=pltpu.CompilerParams(vmem_limit_bytes=24*1024*1024),
        name="attention")(pos,gain,d,*ins)


def pack_kernel(*refs):
    ins, w, wo = refs[:4], refs[4], refs[5]
    for h in range(4):
        w[h * 192 : h * 192 + 192, :] = ins[h][0:192, :]
        wo[h * 64 : h * 64 + 64, :] = ins[h][192:256, :]


def pack(pieces):
    return pl.pallas_call(
        pack_kernel,
        out_shape=[jax.ShapeDtypeStruct((768, 256), bf16), jax.ShapeDtypeStruct((256, 256), bf16)],
        in_specs=[VMEM] * 4,
        out_specs=[VMEM] * 2,
        compiler_params=pltpu.CompilerParams(vmem_limit_bytes=4 * 1024 * 1024),
        name="pack",
    )(*pieces)


def join_kernel(*refs):
    out, sem = refs[4], refs[5]
    copies = [
        pltpu.make_async_copy(refs[i], out.at[pl.ds(i * 256, 256)], sem.at[i]) for i in range(4)
    ]
    for copy in copies:
        copy.start()
    for copy in copies:
        copy.wait()


def join(pieces):
    anywhere = pl.BlockSpec(memory_space=pl.ANY)
    return pl.pallas_call(
        join_kernel,
        out_shape=jax.ShapeDtypeStruct((1024, 256), bf16),
        in_specs=[anywhere] * 4,
        out_specs=anywhere,
        scratch_shapes=[pltpu.SemaphoreType.DMA((4,))],
        name="join",
    )(*pieces)


def proj_block(tok, w, gains, out, at):
    lo = lax.broadcasted_iota(jnp.int32, (BLK, 128), 1) < 64
    half = lax.broadcasted_iota(jnp.int32, (BLK // 2, 128), 1) < 64
    acc = lax.dot_general(tok, w, NT, preferred_element_type=f32)
    for h in range(4):
        qk = acc[:, h * 128 : h * 128 + 128].astype(bf16).astype(f32)
        sq = qk * qk
        s_lo = jnp.sum(jnp.where(lo, sq, 0.0), axis=1, keepdims=True)
        s_hi = jnp.sum(jnp.where(lo, 0.0, sq), axis=1, keepdims=True)
        inv = lax.rsqrt(jnp.where(lo, s_lo, s_hi) * (1 / 64) + 1e-6)
        out[h][at : at + 320, :] = (qk * inv * gains).astype(bf16)
        c = 512 + (h // 2) * 128
        top, bot = acc[:160, c : c + 128], acc[160:, c : c + 128]
        if h % 2:
            top = pltpu.roll(top, 64, 1)
        else:
            bot = pltpu.roll(bot, 64, 1)
        out[h][at + 320 : at + 480, :] = jnp.where(half, top, bot).astype(bf16)


def proj_kernel(idx_ref, gain_ref, *refs, sizes):
    n = sum(sizes)
    toks, ws, outs, w = refs[:n], refs[n : n + 8], refs[n + 8 : n + 12], refs[-1]
    for j in range(8):
        cols = pl.ds(pl.multiple_of(idx_ref[j] * 256, 256), 256)
        for h in range(4):
            w[h * 128 : h * 128 + 128, cols] = ws[j][h * 192 : h * 192 + 128, :]
            w[512 + h * 64 : 576 + h * 64, cols] = ws[j][h * 192 + 128 : h * 192 + 192, :]
    gains = gain_ref[...]
    at = 0
    for b, size in enumerate(sizes):
        parts = [t[...] for t in toks[at : at + size]]
        at += size
        tok = parts[0] if size == 1 else jnp.concatenate(parts, 0)
        proj_block(tok, w[...], gains, outs, b * 480)


def project(cols, gain, blocks, ws):
    toks = [p for block in blocks for p in block]
    return pl.pallas_call(
        functools.partial(proj_kernel, sizes=tuple(len(b) for b in blocks)),
        out_shape=[jax.ShapeDtypeStruct((len(blocks) * 480, 128), bf16)] * 4,
        in_specs=[SMEM] + [VMEM] * (1 + len(toks) + 8),
        out_specs=[VMEM] * 4,
        scratch_shapes=[pltpu.VMEM((768, 2048), bf16)],
        compiler_params=pltpu.CompilerParams(vmem_limit_bytes=20 * 1024 * 1024),
        name="project",
    )(cols, gain, *toks, *ws)


def out_kernel(head_ref, col_ref, heads_ref, *refs):
    ws, o_ref, lhs = refs[:8], refs[8], refs[9]
    half = lax.broadcasted_iota(jnp.int32, (BLK // 2, 128), 1) < 64
    for p in range(8):
        a = heads_ref[head_ref[2 * p]].astype(f32)
        b = heads_ref[head_ref[2 * p + 1]].astype(f32)
        s = slice(p * 128, p * 128 + 128)
        lhs[0:160, s] = jnp.where(half, a, pltpu.roll(b, 64, 1)).astype(bf16)
        lhs[160:320, s] = jnp.where(half, pltpu.roll(a, 64, 1), b).astype(bf16)
    for par in range(2):
        for dx in range(4):
            acc = None
            for dy in range(4):
                rhs = ws[par * 4 + dy][dx * 256 : dx * 256 + 256, :]
                part = lax.dot_general(
                    lhs[:, dy * 256 : dy * 256 + 256], rhs, NN, preferred_element_type=f32
                )
                acc = part if acc is None else acc + part
            cols = pl.ds(pl.multiple_of(col_ref[par * 4 + dx] * 256, 256), 256)
            o_ref[:, cols] = acc.astype(bf16)


def output(order, cols, heads, ws):
    return pl.pallas_call(
        out_kernel,
        out_shape=jax.ShapeDtypeStruct((BLK, 2048), bf16),
        in_specs=[SMEM, SMEM] + [VMEM] * 9,
        out_specs=VMEM,
        scratch_shapes=[pltpu.VMEM((BLK, 1024), bf16)],
        compiler_params=pltpu.CompilerParams(vmem_limit_bytes=12 * 1024 * 1024),
        name="output",
    )(order, cols, heads, *ws)


def turn(step):
    return [(i, (i + step) % 4) for i in range(4)]


def move(value, axis, step):
    pairs = [(0, 1), (1, 0)] if axis == C else turn(step)
    return lax.ppermute(value, axis, pairs)


def spread(value, step):
    pairs = [(2 * i + k, 2 * ((i + (step, -step)[k]) % 4) + k) for i in range(4) for k in (0, 1)]
    return lax.ppermute(value, (Y, C), pairs)


def around(value, axis):
    return [value] + [move(value, axis, -d) for d in (1, 2, 3)]


def on_device(tokens, w_query, w_key, w_value, w_output, qk_gain, decay_sums):
    own = tokens[0]
    z, y, x, c = (lax.axis_index(a) for a in (Z, Y, X, C))
    t1 = spread(own, -1)
    t3 = spread(own, 1)
    t2 = spread(t1, -1)
    near = jnp.where(c == 0, 1, 3)
    piece = jnp.concatenate([w_query.T, w_key.T, w_value.T, w_output], 0)
    w4, wo4 = pack(around(piece, Z))
    ws = around(w4, X)
    ws = ws + [move(w, C, 0) for w in ws]

    cols = jnp.stack(
        [2 * ((x + d) % 4) + e for e in (c, 1 - c) for d in range(4)]
    ).astype(jnp.int32)
    gains = jnp.concatenate([qk_gain[0] * 0.125, qk_gain[1]])[None]
    part0 = project(cols, gains, [[own]], ws)
    part1 = project(cols, gains, [[t1], [t3]], ws)
    part2 = project(cols, gains, [[t2]], ws)
    recv = []
    for part in (part0, part1, part2):
        recv += [part[0]] + [move(part[d], Z, d) for d in (1, 2, 3)]
    ox = around(wo4, X)
    wo16 = join(ox)
    wo = around(wo16, Y)
    sources = [4 * ((z - d) % 4) for d in range(4)]
    pos = [r + y for r in sources]
    pos += [r + (y + e) % 4 for r in sources for e in (near, 4 - near)]
    pos += [r + (y + 2) % 4 for r in sources]
    pos = jnp.stack(pos).astype(jnp.int32)
    heads = attention(pos, gains, decay_sums[0], recv, (1,) * 4 + (2,) * 4 + (1,) * 4)
    heads, *wo = lax.optimization_barrier((heads, *wo))
    wo = wo + [move(w, C, 0) for w in wo]
    merged = lax.all_to_all(heads, SP, 0, 0, tiled=True)
    order = jnp.stack(
        [4 * ((z + d) % 4) + (y + e) % 4 for e in range(4) for d in range(4)]
    ).astype(jnp.int32)
    return output(order, cols, merged, wo)[None]


def solution(mesh):
    torus = Mesh(mesh.devices.reshape(4, 4, 4, 2), ("sp_0", "sp_1", "dp_0", "dp_1"))
    in_specs = (P(DP, SP, None), P(DP, SP), P(DP, SP), P(DP, SP), P(SP, DP), P(), P(DP, SP, None))
    out_specs = P(DP, SP, None)
    return jax.shard_map(
        on_device, mesh=torus, in_specs=in_specs, out_specs=out_specs, check_vma=False
    )
```

```python
import functools

import jax
import jax.numpy as jnp
from jax import lax
from jax.experimental import pallas as pl
from jax.experimental.pallas import tpu as pltpu
from jax.sharding import Mesh
from jax.sharding import PartitionSpec as P


DP = ("dp_0", "dp_1")
SP = ("sp_0", "sp_1")
Z, Y, X, C = "sp_0", "sp_1", "dp_0", "dp_1"
LOG2E = 1.4426950408889634
T = 5120
BLK = 320
BQ = 512
W = 2048
NT = (((1,), (1,)), ((), ()))
NN = (((1,), (0,)), ((), ()))
f32 = jnp.float32
bf16 = jnp.bfloat16
SMEM = pl.BlockSpec(memory_space=pltpu.SMEM)
VMEM = pl.BlockSpec(memory_space=pltpu.VMEM)


def attn_kernel(pos_ref, gain_ref, d_ref, *refs, nblk):
    nin=len(nblk)
    ins=refs[:nin]; out_ref=refs[nin]; ka,qa,vs,vt,ot,rows=refs[nin+1:]
    lane=lax.broadcasted_iota(jnp.int32,(BLK,128),1)
    lo=lane<64
    lanev=lax.broadcasted_iota(jnp.int32,(BLK//2,128),1)
    tail=jnp.where(lanev==64,1.0,0.0)
    n=0
    for a,nb in zip(ins,nblk):
        for b in range(nb):
            base=pl.multiple_of(pos_ref[n]*BLK,64); n+=1
            qk=a[b*480:b*480+320,:].astype(f32)
            rolled=pltpu.roll(qk,64,1)
            ka[pl.ds(base,BLK),0:128]=jnp.where(lo,rolled,qk).astype(bf16)
            qs=jnp.where(lo,qk,rolled)*LOG2E
            hi=qs.astype(bf16).astype(f32)
            qa[pl.ds(base,BLK),0:128]=jnp.where(lo,hi,qs-hi).astype(bf16)
            v=a[b*480+320:b*480+480,:].astype(f32)
            vs[pl.ds(base,BLK//2),:]=jnp.where(lanev<64,v,tail)
            vs[pl.ds(base+BLK//2,BLK//2),:]=jnp.where(lanev<64,pltpu.roll(v,64,1),tail)
    x=jnp.concatenate([d_ref[0:1,i*BQ:(i+1)*BQ] for i in range(T//BQ)]+[jnp.zeros((16-T//BQ,BQ),f32)],0)*LOG2E
    h=x.astype(bf16).astype(f32)
    m=(x-h).astype(bf16).astype(f32)
    l=x-h-m
    dt=jnp.concatenate([-h,-m,-l,h,m,l,jnp.zeros((32,BQ),f32)],0).T
    dl=lax.broadcasted_iota(jnp.int32,(BQ,128),1)
    key_one=jnp.where((dl>=48)&(dl<96),1.0,0.0)
    query_one=jnp.where(dl<48,1.0,0.0)

    def prepare(i):
        s=slice(i*BQ,(i+1)*BQ)
        ka[s,128:256]=jnp.where((dl==i)|(dl==16+i)|(dl==32+i),dt,key_one).astype(bf16)
        qa[s,128:256]=jnp.where((dl==48+i)|(dl==64+i)|(dl==80+i),dt,query_one).astype(bf16)
        vt[:,s]=vs[s,:].T[0:80].astype(bf16)

    def emit(i):
        s=slice(i*BQ,(i+1)*BQ)
        rows[s,0:64]=ot[:,s].T
        for j in range(T//BLK):
            if i*BQ<(j+1)*BLK<=(i+1)*BQ:
                a=rows[j*BLK:j*BLK+160,:]
                b=rows[j*BLK+160:(j+1)*BLK,:]
                out_ref[j]=jnp.where(lanev<64,a,pltpu.roll(b,64,1)).astype(bf16)

    def finish(acc):
        o=acc[0:64]/acc[64:65]
        return o*lax.rsqrt(jnp.mean(o*o,axis=0,keepdims=True)+1e-6)

    def fast():
        kio=lax.broadcasted_iota(jnp.int32,(BQ,BQ),0); qio=lax.broadcasted_iota(jnp.int32,(BQ,BQ),1)
        keep=kio<=qio
        for qi in range(T//BQ):
            q0=qi*BQ
            prepare(qi)
            qb=qa[q0:q0+BQ,:]
            def tile(k0,w,mask):
                s=lax.dot_general(ka[k0:k0+w,:],qb,NT,preferred_element_type=f32)
                p=jnp.exp2(s)
                if mask:
                    p=jnp.where(keep,p,0.0)
                return lax.dot_general(vt[:,k0:k0+w],p.astype(bf16),NN,preferred_element_type=f32)
            acc=tile(q0,BQ,True)
            for k0 in range(0,q0,W):
                acc=acc+tile(k0,min(W,q0-k0),False)
            ot[:,q0:q0+BQ]=finish(acc)
            emit(qi)

    def slow():
        for i in range(T//BQ):
            prepare(i)
        kio=lax.broadcasted_iota(jnp.int32,(BQ,BQ),0); qio=lax.broadcasted_iota(jnp.int32,(BQ,BQ),1)
        def per_q(qi,_):
            q0=pl.multiple_of(qi*BQ,BQ)
            qb=qa[pl.ds(q0,BQ),:]
            def body(j,c):
                m,acc=c
                k0=pl.multiple_of(j*BQ,BQ)
                s=lax.dot_general(ka[pl.ds(k0,BQ),:],qb,NT,preferred_element_type=f32)
                s=jnp.where(kio+k0<=qio+q0,s,-jnp.inf)
                m2=jnp.maximum(m,jnp.max(s,axis=0,keepdims=True))
                p=jnp.exp2(s-m2).astype(bf16)
                acc=acc*jnp.exp2(m-m2)+lax.dot_general(vt[:,pl.ds(k0,BQ)],p,NN,preferred_element_type=f32)
                return m2,acc
            m0=jnp.full((1,BQ),-jnp.inf,f32)
            c=body(qi,(m0,jnp.zeros((80,BQ),f32)))
            _,acc=lax.fori_loop(0,qi,body,c)
            ot[:,pl.ds(q0,BQ)]=finish(acc)
            return 0
        lax.fori_loop(0,T//BQ,per_q,0)
        for i in range(T//BQ):
            emit(i)
    g=jnp.abs(gain_ref[...])
    isfast=jnp.max(g[:,0:64])*jnp.max(g[:,64:128])<=7.7/8
    pl.when(isfast)(fast)
    pl.when(jnp.logical_not(isfast))(slow)


def attention(pos,gain,d,ins,nblk):
    V=pltpu.VMEM
    return pl.pallas_call(functools.partial(attn_kernel,nblk=nblk),
        out_shape=jax.ShapeDtypeStruct((16,160,128),bf16),
        in_specs=[SMEM]+[VMEM]*(2+len(ins)),
        out_specs=VMEM,
        scratch_shapes=[V((T,256),bf16),V((T,256),bf16),V((T,128),f32),V((80,T),bf16),V((64,T),f32),V((T,128),f32)],
        compiler_params=pltpu.CompilerParams(vmem_limit_bytes=24*1024*1024),
        name="attention")(pos,gain,d,*ins)


def pack_kernel(*refs):
    ins, w, wo = refs[:4], refs[4], refs[5]
    for h in range(4):
        w[h * 192 : h * 192 + 192, :] = ins[h][0:192, :]
        wo[h * 64 : h * 64 + 64, :] = ins[h][192:256, :]


def pack(pieces):
    return pl.pallas_call(
        pack_kernel,
        out_shape=[jax.ShapeDtypeStruct((768, 256), bf16), jax.ShapeDtypeStruct((256, 256), bf16)],
        in_specs=[VMEM] * 4,
        out_specs=[VMEM] * 2,
        compiler_params=pltpu.CompilerParams(vmem_limit_bytes=4 * 1024 * 1024),
        name="pack",
    )(*pieces)


def join_kernel(*refs):
    for i in range(4):
        refs[4][i * 256 : i * 256 + 256, :] = refs[i][...]


def join(pieces):
    return pl.pallas_call(
        join_kernel,
        out_shape=jax.ShapeDtypeStruct((1024, 256), bf16),
        in_specs=[VMEM] * 4,
        out_specs=VMEM,
        compiler_params=pltpu.CompilerParams(vmem_limit_bytes=4 * 1024 * 1024),
        name="join",
    )(*pieces)


QK_AT = (0, 256, 384, 512)
V_AT = (128, 192, 640, 704)


def proj_block(tok, w, base, heads, gains, out, at):
    lo = lax.broadcasted_iota(jnp.int32, (BLK, 128), 1) < 64
    half = lax.broadcasted_iota(jnp.int32, (BLK // 2, 128), 1) < 64
    acc = lax.dot_general(tok, w, NT, preferred_element_type=f32)
    for h, dst in zip(heads, out):
        c = QK_AT[h] - base
        qk = acc[:, c : c + 128].astype(bf16).astype(f32)
        sq = qk * qk
        s_lo = jnp.sum(jnp.where(lo, sq, 0.0), axis=1, keepdims=True)
        s_hi = jnp.sum(jnp.where(lo, 0.0, sq), axis=1, keepdims=True)
        inv = lax.rsqrt(jnp.where(lo, s_lo, s_hi) * (1 / 64) + 1e-6)
        dst[at : at + 320, :] = (qk * inv * gains).astype(bf16)
        c = V_AT[h] // 128 * 128 - base
        top, bot = acc[:160, c : c + 128], acc[160:, c : c + 128]
        if h % 2:
            top = pltpu.roll(top, 64, 1)
        else:
            bot = pltpu.roll(bot, 64, 1)
        dst[at + 320 : at + 480, :] = jnp.where(half, top, bot).astype(bf16)


def weights_in_order(idx_ref, ws, w):
    for j in range(8):
        cols = pl.ds(pl.multiple_of(idx_ref[j] * 256, 256), 256)
        for h in range(4):
            w[QK_AT[h] : QK_AT[h] + 128, cols] = ws[j][h * 192 : h * 192 + 128, :]
            w[V_AT[h] : V_AT[h] + 64, cols] = ws[j][h * 192 + 128 : h * 192 + 192, :]


def near_kernel(idx_ref, gain_ref, *refs):
    toks, ws, outs, w = refs[:3], refs[3:11], refs[11:14], refs[14]
    weights_in_order(idx_ref, ws, w)
    gains = gain_ref[...]
    for b in range(3):
        proj_block(toks[b][...], w[128:768], 128, (1, 2, 3), gains, outs, b * 480)


def far_kernel(idx_ref, gain_ref, *refs):
    toks, ws, outs, w = refs[:4], refs[4:12], refs[12:17], refs[17]
    weights_in_order(idx_ref, ws, w)
    gains = gain_ref[...]
    proj_block(toks[0][...], w[...], 0, (0, 1, 2, 3), gains, outs[:4], 0)
    for b in range(3):
        proj_block(toks[b + 1][...], w[0:256], 0, (0,), gains, outs[4:], b * 480)


def project(kernel, lengths, cols, gains, toks, ws):
    return pl.pallas_call(
        kernel,
        out_shape=[jax.ShapeDtypeStruct((n, 128), bf16) for n in lengths],
        in_specs=[SMEM] + [VMEM] * (1 + len(toks) + 8),
        out_specs=[VMEM] * len(lengths),
        scratch_shapes=[pltpu.VMEM((768, 2048), bf16)],
        compiler_params=pltpu.CompilerParams(vmem_limit_bytes=20 * 1024 * 1024),
        name="project",
    )(cols, gains, *toks, *ws)


def out_kernel(head_ref, col_ref, heads_ref, *refs):
    ws, o_ref, lhs = refs[:8], refs[8], refs[9]
    half = lax.broadcasted_iota(jnp.int32, (BLK // 2, 128), 1) < 64
    for p in range(8):
        a = heads_ref[head_ref[2 * p]].astype(f32)
        b = heads_ref[head_ref[2 * p + 1]].astype(f32)
        s = slice(p * 128, p * 128 + 128)
        lhs[0:160, s] = jnp.where(half, a, pltpu.roll(b, 64, 1)).astype(bf16)
        lhs[160:320, s] = jnp.where(half, pltpu.roll(a, 64, 1), b).astype(bf16)
    for par in range(2):
        for dx in range(4):
            acc = None
            for dy in range(4):
                rhs = ws[par * 4 + dy][dx * 256 : dx * 256 + 256, :]
                part = lax.dot_general(
                    lhs[:, dy * 256 : dy * 256 + 256], rhs, NN, preferred_element_type=f32
                )
                acc = part if acc is None else acc + part
            cols = pl.ds(pl.multiple_of(col_ref[par * 4 + dx] * 256, 256), 256)
            o_ref[:, cols] = acc.astype(bf16)


def output(order, cols, heads, ws):
    return pl.pallas_call(
        out_kernel,
        out_shape=jax.ShapeDtypeStruct((BLK, 2048), bf16),
        in_specs=[SMEM, SMEM] + [VMEM] * 9,
        out_specs=VMEM,
        scratch_shapes=[pltpu.VMEM((BLK, 1024), bf16)],
        compiler_params=pltpu.CompilerParams(vmem_limit_bytes=12 * 1024 * 1024),
        name="output",
    )(order, cols, heads, *ws)


def turn(step):
    return [(i, (i + step) % 4) for i in range(4)]


def move(value, axis, step):
    pairs = [(0, 1), (1, 0)] if axis == C else turn(step)
    return lax.ppermute(value, axis, pairs)


def spread(value, axis, step):
    pairs = [(2 * i + k, 2 * ((i + (step, -step)[k]) % 4) + k) for i in range(4) for k in (0, 1)]
    return lax.ppermute(value, (axis, C), pairs)


def around(value, axis):
    return [value] + [move(value, axis, -d) for d in (1, 2, 3)]


def on_device(tokens, w_query, w_key, w_value, w_output, qk_gain, decay_sums):
    own = tokens[0]
    z, y, x, c = (lax.axis_index(a) for a in (Z, Y, X, C))
    t1 = spread(own, Y, -1)
    t3 = spread(own, Y, 1)
    t2 = spread(t1, Y, -1)
    piece = jnp.concatenate([w_query.T, w_key.T, w_value.T, w_output], 0)
    w4, wo4 = pack(around(piece, Z))
    w1 = spread(w4, X, -1)
    ws = [w4, w1, spread(w4, X, 1), spread(w1, X, -1)]
    ws = ws + [move(w, C, 0) for w in ws]

    near = jnp.where(c == 0, 1, 3)
    turns = [(c, (0, near, 4 - near, 2)), (1 - c, (0, 4 - near, near, 2))]
    cols = jnp.stack([2 * ((x + d) % 4) + e for e, ds in turns for d in ds]).astype(jnp.int32)
    out_cols = jnp.stack(
        [2 * ((x + d) % 4) + e for e in (c, 1 - c) for d in range(4)]
    ).astype(jnp.int32)
    gains = jnp.concatenate([qk_gain[0] * 0.125, qk_gain[1]])[None]
    near_toks = [own, t1, t3]
    part1 = project(near_kernel, (1440,) * 3, cols, gains, near_toks, ws)
    *part1, wo4 = lax.optimization_barrier((*part1, wo4))
    *part2, mine = project(
        far_kernel, (480,) * 4 + (1440,), cols, gains, [t2] + near_toks, ws
    )
    recv = []
    for part in ([mine] + part1, part2):
        recv += [part[0]] + [move(part[d], Z, d) for d in (1, 2, 3)]
    wo16 = join(around(wo4, X))
    wo = around(wo16, Y)
    pos = [4 * ((z - d) % 4) + (y + e) % 4 for d in range(4) for e in (0, near, 4 - near)]
    pos += [4 * ((z - d) % 4) + (y + 2) % 4 for d in range(4)]
    pos = jnp.stack(pos).astype(jnp.int32)
    heads = attention(pos, gains, decay_sums[0], recv, (3, 3, 3, 3, 1, 1, 1, 1))
    heads, *wo = lax.optimization_barrier((heads, *wo))
    wo = wo + [move(w, C, 0) for w in wo]
    merged = lax.all_to_all(heads, SP, 0, 0, tiled=True)
    order = jnp.stack(
        [4 * ((z + d) % 4) + (y + e) % 4 for e in range(4) for d in range(4)]
    ).astype(jnp.int32)
    return output(order, out_cols, merged, wo)[None]


def solution(mesh):
    torus = Mesh(mesh.devices.reshape(4, 4, 4, 2), ("sp_0", "sp_1", "dp_0", "dp_1"))
    in_specs = (P(DP, SP, None), P(DP, SP), P(DP, SP), P(DP, SP), P(SP, DP), P(), P(DP, SP, None))
    out_specs = P(DP, SP, None)
    return jax.shard_map(
        on_device, mesh=torus, in_specs=in_specs, out_specs=out_specs, check_vma=False
    )
```

```python
import functools

import jax
import jax.numpy as jnp
from jax import lax
from jax.experimental import pallas as pl
from jax.experimental.pallas import tpu as pltpu
from jax.sharding import Mesh
from jax.sharding import PartitionSpec as P


DP = ("dp_0", "dp_1")
SP = ("sp_0", "sp_1")
Z, Y, X, C = "sp_0", "sp_1", "dp_0", "dp_1"
LOG2E = 1.4426950408889634
T = 5120
BLK = 320
BQ = 512
W = 2048
NT = (((1,), (1,)), ((), ()))
NN = (((1,), (0,)), ((), ()))
f32 = jnp.float32
bf16 = jnp.bfloat16
SMEM = pl.BlockSpec(memory_space=pltpu.SMEM)
VMEM = pl.BlockSpec(memory_space=pltpu.VMEM)


def attn_kernel(pos_ref, gain_ref, d_ref, *refs, nblk):
    nin=len(nblk)
    ins=refs[:nin]; out_ref=refs[nin]; ka,qa,vs,vt,ot,rows=refs[nin+1:]
    lane=lax.broadcasted_iota(jnp.int32,(BLK,128),1)
    lo=lane<64
    lanev=lax.broadcasted_iota(jnp.int32,(BLK//2,128),1)
    tail=jnp.where(lanev==64,1.0,0.0)
    n=0
    for a,nb in zip(ins,nblk):
        for b in range(nb):
            base=pl.multiple_of(pos_ref[n]*BLK,64); n+=1
            qk=a[b*480:b*480+320,:].astype(f32)
            rolled=pltpu.roll(qk,64,1)
            ka[pl.ds(base,BLK),0:128]=jnp.where(lo,rolled,qk).astype(bf16)
            qs=jnp.where(lo,qk,rolled)*LOG2E
            hi=qs.astype(bf16).astype(f32)
            qa[pl.ds(base,BLK),0:128]=jnp.where(lo,hi,qs-hi).astype(bf16)
            v=a[b*480+320:b*480+480,:].astype(f32)
            vs[pl.ds(base,BLK//2),:]=jnp.where(lanev<64,v,tail)
            vs[pl.ds(base+BLK//2,BLK//2),:]=jnp.where(lanev<64,pltpu.roll(v,64,1),tail)
    x=jnp.concatenate([d_ref[0:1,i*BQ:(i+1)*BQ] for i in range(T//BQ)]+[jnp.zeros((16-T//BQ,BQ),f32)],0)*LOG2E
    h=x.astype(bf16).astype(f32)
    m=(x-h).astype(bf16).astype(f32)
    l=x-h-m
    dt=jnp.concatenate([-h,-m,-l,h,m,l,jnp.zeros((32,BQ),f32)],0).T
    dl=lax.broadcasted_iota(jnp.int32,(BQ,128),1)
    key_one=jnp.where((dl>=48)&(dl<96),1.0,0.0)
    query_one=jnp.where(dl<48,1.0,0.0)

    def prepare(i):
        s=slice(i*BQ,(i+1)*BQ)
        ka[s,128:256]=jnp.where((dl==i)|(dl==16+i)|(dl==32+i),dt,key_one).astype(bf16)
        qa[s,128:256]=jnp.where((dl==48+i)|(dl==64+i)|(dl==80+i),dt,query_one).astype(bf16)
        vt[:,s]=vs[s,:].T[0:80].astype(bf16)

    def emit(i):
        s=slice(i*BQ,(i+1)*BQ)
        rows[s,0:64]=ot[:,s].T
        for j in range(T//BLK):
            if i*BQ<(j+1)*BLK<=(i+1)*BQ:
                a=rows[j*BLK:j*BLK+160,:]
                b=rows[j*BLK+160:(j+1)*BLK,:]
                out_ref[j]=jnp.where(lanev<64,a,pltpu.roll(b,64,1)).astype(bf16)

    def finish(acc):
        o=acc[0:64]/acc[64:65]
        return o*lax.rsqrt(jnp.mean(o*o,axis=0,keepdims=True)+1e-6)

    def fast():
        kio=lax.broadcasted_iota(jnp.int32,(BQ,BQ),0); qio=lax.broadcasted_iota(jnp.int32,(BQ,BQ),1)
        keep=kio<=qio
        for qi in range(T//BQ):
            q0=qi*BQ
            prepare(qi)
            qb=qa[q0:q0+BQ,:]

            def tile(k0,w,mask):
                s=lax.dot_general(ka[k0:k0+w,:],qb,NT,preferred_element_type=f32)
                p=jnp.exp2(s)
                if mask:
                    p=jnp.where(keep,p,0.0)
                return lax.dot_general(vt[:,k0:k0+w],p.astype(bf16),NN,preferred_element_type=f32)

            acc=tile(q0,BQ,True)
            for k0 in range(0,q0,W):
                acc=acc+tile(k0,min(W,q0-k0),False)
            ot[:,q0:q0+BQ]=finish(acc)
            emit(qi)

    def slow():
        for i in range(T//BQ):
            prepare(i)
        kio=lax.broadcasted_iota(jnp.int32,(BQ,BQ),0); qio=lax.broadcasted_iota(jnp.int32,(BQ,BQ),1)

        def per_q(qi,_):
            q0=pl.multiple_of(qi*BQ,BQ)
            qb=qa[pl.ds(q0,BQ),:]

            def body(j,c):
                m,acc=c
                k0=pl.multiple_of(j*BQ,BQ)
                s=lax.dot_general(ka[pl.ds(k0,BQ),:],qb,NT,preferred_element_type=f32)
                s=jnp.where(kio+k0<=qio+q0,s,-jnp.inf)
                m2=jnp.maximum(m,jnp.max(s,axis=0,keepdims=True))
                p=jnp.exp2(s-m2).astype(bf16)
                acc=acc*jnp.exp2(m-m2)+lax.dot_general(vt[:,pl.ds(k0,BQ)],p,NN,preferred_element_type=f32)
                return m2,acc

            m0=jnp.full((1,BQ),-jnp.inf,f32)
            c=body(qi,(m0,jnp.zeros((80,BQ),f32)))
            _,acc=lax.fori_loop(0,qi,body,c)
            ot[:,pl.ds(q0,BQ)]=finish(acc)
            return 0

        lax.fori_loop(0,T//BQ,per_q,0)
        for i in range(T//BQ):
            emit(i)

    g=jnp.abs(gain_ref[...])
    isfast=jnp.max(g[:,0:64])*jnp.max(g[:,64:128])<=7.7/8
    pl.when(isfast)(fast)
    pl.when(jnp.logical_not(isfast))(slow)


def attention(pos,gain,d,ins,nblk):
    V=pltpu.VMEM
    return pl.pallas_call(functools.partial(attn_kernel,nblk=nblk),
        out_shape=jax.ShapeDtypeStruct((16,160,128),bf16),
        in_specs=[SMEM]+[VMEM]*(2+len(ins)),
        out_specs=VMEM,
        scratch_shapes=[V((T,256),bf16),V((T,256),bf16),V((T,128),f32),V((80,T),bf16),V((64,T),f32),V((T,128),f32)],
        compiler_params=pltpu.CompilerParams(vmem_limit_bytes=24*1024*1024),
        name="attention")(pos,gain,d,*ins)


def pack_kernel(*refs):
    ins, w, wo = refs[:4], refs[4], refs[5]
    for h in range(4):
        w[h * 192 : h * 192 + 192, :] = ins[h][0:192, :]
        wo[h * 64 : h * 64 + 64, :] = ins[h][192:256, :]


def pack(pieces):
    return pl.pallas_call(
        pack_kernel,
        out_shape=[jax.ShapeDtypeStruct((768, 256), bf16), jax.ShapeDtypeStruct((256, 256), bf16)],
        in_specs=[VMEM] * 4,
        out_specs=[VMEM] * 2,
        compiler_params=pltpu.CompilerParams(vmem_limit_bytes=4 * 1024 * 1024),
        name="pack",
    )(*pieces)


def join_kernel(*refs):
    for i in range(4):
        refs[4][i * 256 : i * 256 + 256, :] = refs[i][...]


def join(pieces):
    return pl.pallas_call(
        join_kernel,
        out_shape=jax.ShapeDtypeStruct((1024, 256), bf16),
        in_specs=[VMEM] * 4,
        out_specs=VMEM,
        compiler_params=pltpu.CompilerParams(vmem_limit_bytes=4 * 1024 * 1024),
        name="join",
    )(*pieces)


def proj_block(tok, w, gains, out, at):
    lo = lax.broadcasted_iota(jnp.int32, (BLK, 128), 1) < 64
    half = lax.broadcasted_iota(jnp.int32, (BLK // 2, 128), 1) < 64
    acc = lax.dot_general(tok, w, NT, preferred_element_type=f32)
    for h in range(4):
        qk = acc[:, h * 128 : h * 128 + 128].astype(bf16).astype(f32)
        sq = qk * qk
        s_lo = jnp.sum(jnp.where(lo, sq, 0.0), axis=1, keepdims=True)
        s_hi = jnp.sum(jnp.where(lo, 0.0, sq), axis=1, keepdims=True)
        inv = lax.rsqrt(jnp.where(lo, s_lo, s_hi) * (1 / 64) + 1e-6)
        out[h][at : at + 320, :] = (qk * inv * gains).astype(bf16)
        c = 512 + (h // 2) * 128
        top, bot = acc[:160, c : c + 128], acc[160:, c : c + 128]
        if h % 2:
            top = pltpu.roll(top, 64, 1)
        else:
            bot = pltpu.roll(bot, 64, 1)
        out[h][at + 320 : at + 480, :] = jnp.where(half, top, bot).astype(bf16)


def proj_kernel(idx_ref, gain_ref, *refs, sizes):
    n = sum(sizes)
    toks, ws, outs, w = refs[:n], refs[n : n + 8], refs[n + 8 : n + 12], refs[-1]
    for j in range(8):
        cols = pl.ds(pl.multiple_of(idx_ref[j] * 256, 256), 256)
        for h in range(4):
            w[h * 128 : h * 128 + 128, cols] = ws[j][h * 192 : h * 192 + 128, :]
            w[512 + h * 64 : 576 + h * 64, cols] = ws[j][h * 192 + 128 : h * 192 + 192, :]
    gains = gain_ref[...]
    at = 0
    for b, size in enumerate(sizes):
        parts = [t[...] for t in toks[at : at + size]]
        at += size
        tok = parts[0] if size == 1 else jnp.concatenate(parts, 0)
        proj_block(tok, w[...], gains, outs, b * 480)


def project(cols, gain, blocks, ws):
    toks = [p for block in blocks for p in block]
    return pl.pallas_call(
        functools.partial(proj_kernel, sizes=tuple(len(b) for b in blocks)),
        out_shape=[jax.ShapeDtypeStruct((len(blocks) * 480, 128), bf16)] * 4,
        in_specs=[SMEM] + [VMEM] * (1 + len(toks) + 8),
        out_specs=[VMEM] * 4,
        scratch_shapes=[pltpu.VMEM((768, 2048), bf16)],
        compiler_params=pltpu.CompilerParams(vmem_limit_bytes=20 * 1024 * 1024),
        name="project",
    )(cols, gain, *toks, *ws)


def out_kernel(head_ref, col_ref, heads_ref, *refs):
    ws, o_ref, lhs = refs[:8], refs[8], refs[9]
    i = pl.program_id(0)

    @pl.when(i == 0)
    def _():
        half = lax.broadcasted_iota(jnp.int32, (BLK // 2, 128), 1) < 64
        for p in range(8):
            a = heads_ref[head_ref[2 * p]].astype(f32)
            b = heads_ref[head_ref[2 * p + 1]].astype(f32)
            s = slice(p * 128, p * 128 + 128)
            lhs[0:160, s] = jnp.where(half, a, pltpu.roll(b, 64, 1)).astype(bf16)
            lhs[160:320, s] = jnp.where(half, pltpu.roll(a, 64, 1), b).astype(bf16)

    for par in range(2):
        acc = None
        for dy in range(4):
            part = lax.dot_general(
                lhs[:, dy * 256 : dy * 256 + 256], ws[par * 4 + dy][...], NN, preferred_element_type=f32
            )
            acc = part if acc is None else acc + part
        side = col_ref[par * 4 + i] % 2
        o_ref[:, pl.ds(pl.multiple_of(side * 256, 256), 256)] = acc.astype(bf16)


def output(order, cols, heads, ws):
    return pl.pallas_call(
        out_kernel,
        out_shape=jax.ShapeDtypeStruct((BLK, 2048), bf16),
        grid_spec=pltpu.PrefetchScalarGridSpec(
            num_scalar_prefetch=2,
            grid=(4,),
            in_specs=[pl.BlockSpec((16, 160, 128), lambda i, order, cols: (0, 0, 0))]
            + [pl.BlockSpec((256, 256), lambda i, order, cols: (i, 0))] * 8,
            out_specs=pl.BlockSpec((BLK, 512), lambda i, order, cols: (0, cols[i] // 2)),
            scratch_shapes=[pltpu.VMEM((BLK, 1024), bf16)],
        ),
        compiler_params=pltpu.CompilerParams(vmem_limit_bytes=12 * 1024 * 1024),
        name="output",
    )(order, cols, heads, *ws)


def turn(step):
    return [(i, (i + step) % 4) for i in range(4)]


def move(value, axis, step):
    pairs = [(0, 1), (1, 0)] if axis == C else turn(step)
    return lax.ppermute(value, axis, pairs)


def spread(value, axis, step):
    pairs = [(2 * i + k, 2 * ((i + (step, -step)[k]) % 4) + k) for i in range(4) for k in (0, 1)]
    return lax.ppermute(value, (axis, C), pairs)


def around(value, axis):
    return [value] + [move(value, axis, -d) for d in (1, 2, 3)]


def on_device(tokens, w_query, w_key, w_value, w_output, qk_gain, decay_sums):
    own = tokens[0]
    z, y, x, c = (lax.axis_index(a) for a in (Z, Y, X, C))
    t1 = spread(own, Y, -1)
    t3 = spread(own, Y, 1)
    t2 = spread(t1, Y, -1)
    piece = jnp.concatenate([w_query.T, w_key.T, w_value.T, w_output], 0)
    w4, wo4 = pack(around(piece, Z))
    w1 = spread(w4, X, -1)
    ws = [w4, w1, spread(w4, X, 1), spread(w1, X, -1)]
    ws = ws + [move(w, C, 0) for w in ws]

    near = jnp.where(c == 0, 1, 3)
    turns = [(c, (0, near, 4 - near, 2)), (1 - c, (0, 4 - near, near, 2))]
    cols = jnp.stack([2 * ((x + d) % 4) + e for e, ds in turns for d in ds]).astype(jnp.int32)
    out_cols = jnp.stack(
        [2 * ((x + d) % 4) + e for e in (c, 1 - c) for d in range(4)]
    ).astype(jnp.int32)
    gains = jnp.concatenate([qk_gain[0] * 0.125, qk_gain[1]])[None]
    part1 = project(cols, gains, [[own], [t1], [t3]], ws)
    *part1, wo4 = lax.optimization_barrier((*part1, wo4))
    part2 = project(cols, gains, [[t2]], ws)
    recv = []
    for part in (part1, part2):
        recv += [part[0]] + [move(part[d], Z, d) for d in (1, 2, 3)]
    wo16 = join(around(wo4, X))
    wo = around(wo16, Y)
    pos = [4 * ((z - d) % 4) + (y + e) % 4 for d in range(4) for e in (0, near, 4 - near)]
    pos += [4 * ((z - d) % 4) + (y + 2) % 4 for d in range(4)]
    pos = jnp.stack(pos).astype(jnp.int32)
    heads = attention(pos, gains, decay_sums[0], recv, (3, 3, 3, 3, 1, 1, 1, 1))
    heads, *wo = lax.optimization_barrier((heads, *wo))
    wo = wo + [move(w, C, 0) for w in wo]
    merged = lax.all_to_all(heads, SP, 0, 0, tiled=True)
    order = jnp.stack(
        [4 * ((z + d) % 4) + (y + e) % 4 for e in range(4) for d in range(4)]
    ).astype(jnp.int32)
    return output(order, out_cols, merged, wo)[None]


def solution(mesh):
    torus = Mesh(mesh.devices.reshape(4, 4, 4, 2), ("sp_0", "sp_1", "dp_0", "dp_1"))
    in_specs = (P(DP, SP, None), P(DP, SP), P(DP, SP), P(DP, SP), P(SP, DP), P(), P(DP, SP, None))
    out_specs = P(DP, SP, None)
    return jax.shard_map(
        on_device, mesh=torus, in_specs=in_specs, out_specs=out_specs, check_vma=False
    )
```

```python
import functools

import jax
import jax.numpy as jnp
from jax import lax
from jax.experimental import pallas as pl
from jax.experimental.pallas import tpu as pltpu
from jax.sharding import Mesh
from jax.sharding import PartitionSpec as P


DP = ("dp_0", "dp_1")
SP = ("sp_0", "sp_1")
Z, Y, X, C = "sp_0", "sp_1", "dp_0", "dp_1"
LOG2E = 1.4426950408889634
T = 5120
BLK = 320
BQ = 512
W = 5120
NT = (((1,), (1,)), ((), ()))
NN = (((1,), (0,)), ((), ()))
f32 = jnp.float32
bf16 = jnp.bfloat16
SMEM = pl.BlockSpec(memory_space=pltpu.SMEM)
VMEM = pl.BlockSpec(memory_space=pltpu.VMEM)


def attn_kernel(pos_ref, gain_ref, d_ref, *refs, nblk):
    nin=len(nblk)
    ins=refs[:nin]; out_ref=refs[nin]; ka,qa,vs,vt,ot,rows=refs[nin+1:]
    lane=lax.broadcasted_iota(jnp.int32,(BLK,128),1)
    lo=lane<64
    lanev=lax.broadcasted_iota(jnp.int32,(BLK//2,128),1)
    tail=jnp.where(lanev==64,1.0,0.0)
    n=0
    for a,nb in zip(ins,nblk):
        for b in range(nb):
            base=pl.multiple_of(pos_ref[n]*BLK,64); n+=1
            qk=a[b*480:b*480+320,:].astype(f32)
            rolled=pltpu.roll(qk,64,1)
            ka[pl.ds(base,BLK),0:128]=jnp.where(lo,rolled,qk).astype(bf16)
            qs=jnp.where(lo,qk,rolled)*LOG2E
            hi=qs.astype(bf16).astype(f32)
            qa[pl.ds(base,BLK),0:128]=jnp.where(lo,hi,qs-hi).astype(bf16)
            v=a[b*480+320:b*480+480,:].astype(f32)
            vs[pl.ds(base,BLK//2),:]=jnp.where(lanev<64,v,tail)
            vs[pl.ds(base+BLK//2,BLK//2),:]=jnp.where(lanev<64,pltpu.roll(v,64,1),tail)
    x=jnp.concatenate([d_ref[0:1,i*BQ:(i+1)*BQ] for i in range(T//BQ)]+[jnp.zeros((16-T//BQ,BQ),f32)],0)*LOG2E
    h=x.astype(bf16).astype(f32)
    m=(x-h).astype(bf16).astype(f32)
    l=x-h-m
    dt=jnp.concatenate([-h,-m,-l,h,m,l,jnp.zeros((32,BQ),f32)],0).T
    dl=lax.broadcasted_iota(jnp.int32,(BQ,128),1)
    key_one=jnp.where((dl>=48)&(dl<96),1.0,0.0)
    query_one=jnp.where(dl<48,1.0,0.0)

    def prepare(i):
        s=slice(i*BQ,(i+1)*BQ)
        ka[s,128:256]=jnp.where((dl==i)|(dl==16+i)|(dl==32+i),dt,key_one).astype(bf16)
        qa[s,128:256]=jnp.where((dl==48+i)|(dl==64+i)|(dl==80+i),dt,query_one).astype(bf16)
        vt[:,s]=vs[s,:].T[0:80].astype(bf16)

    def emit(i):
        s=slice(i*BQ,(i+1)*BQ)
        rows[s,0:64]=ot[:,s].T
        for j in range(T//BLK):
            if i*BQ<(j+1)*BLK<=(i+1)*BQ:
                a=rows[j*BLK:j*BLK+160,:]
                b=rows[j*BLK+160:(j+1)*BLK,:]
                out_ref[j]=jnp.where(lanev<64,a,pltpu.roll(b,64,1)).astype(bf16)

    def finish(acc):
        o=acc[0:64]/acc[64:65]
        return o*lax.rsqrt(jnp.mean(o*o,axis=0,keepdims=True)+1e-6)

    def fast():
        kio=lax.broadcasted_iota(jnp.int32,(BQ,BQ),0); qio=lax.broadcasted_iota(jnp.int32,(BQ,BQ),1)
        keep=kio<=qio
        for qi in range(T//BQ):
            q0=qi*BQ
            prepare(qi)
            qb=qa[q0:q0+BQ,:]
            def tile(k0,w,mask):
                s=lax.dot_general(ka[k0:k0+w,:],qb,NT,preferred_element_type=f32)
                p=jnp.exp2(s)
                if mask:
                    p=jnp.where(keep,p,0.0)
                return lax.dot_general(vt[:,k0:k0+w],p.astype(bf16),NN,preferred_element_type=f32)
            acc=tile(q0,BQ,True)
            for k0 in range(0,q0,W):
                acc=acc+tile(k0,min(W,q0-k0),False)
            ot[:,q0:q0+BQ]=finish(acc)
            emit(qi)

    def slow():
        for i in range(T//BQ):
            prepare(i)
        kio=lax.broadcasted_iota(jnp.int32,(BQ,BQ),0); qio=lax.broadcasted_iota(jnp.int32,(BQ,BQ),1)
        def per_q(qi,_):
            q0=pl.multiple_of(qi*BQ,BQ)
            qb=qa[pl.ds(q0,BQ),:]
            def body(j,c):
                m,acc=c
                k0=pl.multiple_of(j*BQ,BQ)
                s=lax.dot_general(ka[pl.ds(k0,BQ),:],qb,NT,preferred_element_type=f32)
                s=jnp.where(kio+k0<=qio+q0,s,-jnp.inf)
                m2=jnp.maximum(m,jnp.max(s,axis=0,keepdims=True))
                p=jnp.exp2(s-m2).astype(bf16)
                acc=acc*jnp.exp2(m-m2)+lax.dot_general(vt[:,pl.ds(k0,BQ)],p,NN,preferred_element_type=f32)
                return m2,acc
            m0=jnp.full((1,BQ),-jnp.inf,f32)
            c=body(qi,(m0,jnp.zeros((80,BQ),f32)))
            _,acc=lax.fori_loop(0,qi,body,c)
            ot[:,pl.ds(q0,BQ)]=finish(acc)
            return 0
        lax.fori_loop(0,T//BQ,per_q,0)
        for i in range(T//BQ):
            emit(i)
    g=jnp.abs(gain_ref[...])
    isfast=jnp.max(g[:,0:64])*jnp.max(g[:,64:128])<=7.7/8
    pl.when(isfast)(fast)
    pl.when(jnp.logical_not(isfast))(slow)


def attention(pos,gain,d,ins,nblk):
    V=pltpu.VMEM
    return pl.pallas_call(functools.partial(attn_kernel,nblk=nblk),
        out_shape=jax.ShapeDtypeStruct((16,160,128),bf16),
        in_specs=[SMEM]+[VMEM]*(2+len(ins)),
        out_specs=VMEM,
        scratch_shapes=[V((T,256),bf16),V((T,256),bf16),V((T,128),f32),V((80,T),bf16),V((64,T),f32),V((T,128),f32)],
        compiler_params=pltpu.CompilerParams(vmem_limit_bytes=24*1024*1024),
        name="attention")(pos,gain,d,*ins)


def pack_kernel(*refs):
    ins, w, wo = refs[:4], refs[4], refs[5]
    for h in range(4):
        w[h * 192 : h * 192 + 192, :] = ins[h][0:192, :]
        wo[h * 64 : h * 64 + 64, :] = ins[h][192:256, :]


def pack(pieces):
    return pl.pallas_call(
        pack_kernel,
        out_shape=[jax.ShapeDtypeStruct((768, 256), bf16), jax.ShapeDtypeStruct((256, 256), bf16)],
        in_specs=[VMEM] * 4,
        out_specs=[VMEM] * 2,
        compiler_params=pltpu.CompilerParams(vmem_limit_bytes=4 * 1024 * 1024),
        name="pack",
    )(*pieces)


def join_kernel(*refs):
    for i in range(4):
        refs[4][i * 256 : i * 256 + 256, :] = refs[i][...]


def join(pieces):
    return pl.pallas_call(
        join_kernel,
        out_shape=jax.ShapeDtypeStruct((1024, 256), bf16),
        in_specs=[VMEM] * 4,
        out_specs=VMEM,
        compiler_params=pltpu.CompilerParams(vmem_limit_bytes=4 * 1024 * 1024),
        name="join",
    )(*pieces)


def proj_block(tok, w, gains, out, at):
    lo = lax.broadcasted_iota(jnp.int32, (BLK, 128), 1) < 64
    half = lax.broadcasted_iota(jnp.int32, (BLK // 2, 128), 1) < 64
    acc = lax.dot_general(tok, w, NT, preferred_element_type=f32)
    for h in range(4):
        qk = acc[:, h * 128 : h * 128 + 128].astype(bf16).astype(f32)
        sq = qk * qk
        s_lo = jnp.sum(jnp.where(lo, sq, 0.0), axis=1, keepdims=True)
        s_hi = jnp.sum(jnp.where(lo, 0.0, sq), axis=1, keepdims=True)
        inv = lax.rsqrt(jnp.where(lo, s_lo, s_hi) * (1 / 64) + 1e-6)
        out[h][at : at + 320, :] = (qk * inv * gains).astype(bf16)
        c = 512 + (h // 2) * 128
        top, bot = acc[:160, c : c + 128], acc[160:, c : c + 128]
        if h % 2:
            top = pltpu.roll(top, 64, 1)
        else:
            bot = pltpu.roll(bot, 64, 1)
        out[h][at + 320 : at + 480, :] = jnp.where(half, top, bot).astype(bf16)


def proj_kernel(idx_ref, gain_ref, *refs, sizes):
    n = sum(sizes)
    toks, ws, outs, w = refs[:n], refs[n : n + 8], refs[n + 8 : n + 12], refs[-1]
    for j in range(8):
        cols = pl.ds(pl.multiple_of(idx_ref[j] * 256, 256), 256)
        for h in range(4):
            w[h * 128 : h * 128 + 128, cols] = ws[j][h * 192 : h * 192 + 128, :]
            w[512 + h * 64 : 576 + h * 64, cols] = ws[j][h * 192 + 128 : h * 192 + 192, :]
    gains = gain_ref[...]
    at = 0
    for b, size in enumerate(sizes):
        parts = [t[...] for t in toks[at : at + size]]
        at += size
        tok = parts[0] if size == 1 else jnp.concatenate(parts, 0)
        proj_block(tok, w[...], gains, outs, b * 480)


def project(cols, gain, blocks, ws):
    toks = [p for block in blocks for p in block]
    return pl.pallas_call(
        functools.partial(proj_kernel, sizes=tuple(len(b) for b in blocks)),
        out_shape=[jax.ShapeDtypeStruct((len(blocks) * 480, 128), bf16)] * 4,
        in_specs=[SMEM] + [VMEM] * (1 + len(toks) + 8),
        out_specs=[VMEM] * 4,
        scratch_shapes=[pltpu.VMEM((768, 2048), bf16)],
        compiler_params=pltpu.CompilerParams(vmem_limit_bytes=20 * 1024 * 1024),
        name="project",
    )(cols, gain, *toks, *ws)


def out_kernel(head_ref, col_ref, heads_ref, *refs):
    ws, o_ref, lhs = refs[:8], refs[8], refs[9]
    half = lax.broadcasted_iota(jnp.int32, (BLK // 2, 128), 1) < 64
    for p in range(8):
        a = heads_ref[head_ref[2 * p]].astype(f32)
        b = heads_ref[head_ref[2 * p + 1]].astype(f32)
        s = slice(p * 128, p * 128 + 128)
        lhs[0:160, s] = jnp.where(half, a, pltpu.roll(b, 64, 1)).astype(bf16)
        lhs[160:320, s] = jnp.where(half, pltpu.roll(a, 64, 1), b).astype(bf16)
    for par in range(2):
        for dx in range(4):
            acc = None
            for dy in range(4):
                rhs = ws[par * 4 + dy][dx * 256 : dx * 256 + 256, :]
                part = lax.dot_general(
                    lhs[:, dy * 256 : dy * 256 + 256], rhs, NN, preferred_element_type=f32
                )
                acc = part if acc is None else acc + part
            cols = pl.ds(pl.multiple_of(col_ref[par * 4 + dx] * 256, 256), 256)
            o_ref[:, cols] = acc.astype(bf16)


def output(order, cols, heads, ws):
    return pl.pallas_call(
        out_kernel,
        out_shape=jax.ShapeDtypeStruct((BLK, 2048), bf16),
        in_specs=[SMEM, SMEM] + [VMEM] * 9,
        out_specs=VMEM,
        scratch_shapes=[pltpu.VMEM((BLK, 1024), bf16)],
        compiler_params=pltpu.CompilerParams(vmem_limit_bytes=12 * 1024 * 1024),
        name="output",
    )(order, cols, heads, *ws)


def turn(step):
    return [(i, (i + step) % 4) for i in range(4)]


def move(value, axis, step):
    pairs = [(0, 1), (1, 0)] if axis == C else turn(step)
    return lax.ppermute(value, axis, pairs)


def spread(value, axis, step):
    pairs = [(2 * i + k, 2 * ((i + (step, -step)[k]) % 4) + k) for i in range(4) for k in (0, 1)]
    return lax.ppermute(value, (axis, C), pairs)


def around(value, axis):
    return [value] + [move(value, axis, -d) for d in (1, 2, 3)]


def on_device(tokens, w_query, w_key, w_value, w_output, qk_gain, decay_sums):
    own = tokens[0]
    z, y, x, c = (lax.axis_index(a) for a in (Z, Y, X, C))
    t1 = spread(own, Y, -1)
    t3 = spread(own, Y, 1)
    t2 = spread(t1, Y, -1)
    piece = jnp.concatenate([w_query.T, w_key.T, w_value.T, w_output], 0)
    w4, wo4 = pack(around(piece, Z))
    w1 = spread(w4, X, -1)
    ws = [w4, w1, spread(w4, X, 1), spread(w1, X, -1)]
    ws = ws + [move(w, C, 0) for w in ws]

    near = jnp.where(c == 0, 1, 3)
    turns = [(c, (0, near, 4 - near, 2)), (1 - c, (0, 4 - near, near, 2))]
    cols = jnp.stack([2 * ((x + d) % 4) + e for e, ds in turns for d in ds]).astype(jnp.int32)
    out_cols = jnp.stack(
        [2 * ((x + d) % 4) + e for e in (c, 1 - c) for d in range(4)]
    ).astype(jnp.int32)
    gains = jnp.concatenate([qk_gain[0] * 0.125, qk_gain[1]])[None]
    part1 = project(cols, gains, [[own], [t1], [t3]], ws)
    *part1, wo4 = lax.optimization_barrier((*part1, wo4))
    part2 = project(cols, gains, [[t2]], ws)
    recv = []
    for part in (part1, part2):
        recv += [part[0]] + [move(part[d], Z, d) for d in (1, 2, 3)]
    wo16 = join(around(wo4, X))
    wo = around(wo16, Y)
    pos = [4 * ((z - d) % 4) + (y + e) % 4 for d in range(4) for e in (0, near, 4 - near)]
    pos += [4 * ((z - d) % 4) + (y + 2) % 4 for d in range(4)]
    pos = jnp.stack(pos).astype(jnp.int32)
    heads = attention(pos, gains, decay_sums[0], recv, (3, 3, 3, 3, 1, 1, 1, 1))
    heads, *wo = lax.optimization_barrier((heads, *wo))
    wo = wo + [move(w, C, 0) for w in wo]
    merged = lax.all_to_all(heads, SP, 0, 0, tiled=True)
    order = jnp.stack(
        [4 * ((z + d) % 4) + (y + e) % 4 for e in range(4) for d in range(4)]
    ).astype(jnp.int32)
    return output(order, out_cols, merged, wo)[None]


def solution(mesh):
    torus = Mesh(mesh.devices.reshape(4, 4, 4, 2), ("sp_0", "sp_1", "dp_0", "dp_1"))
    in_specs = (P(DP, SP, None), P(DP, SP), P(DP, SP), P(DP, SP), P(SP, DP), P(), P(DP, SP, None))
    out_specs = P(DP, SP, None)
    return jax.shard_map(
        on_device, mesh=torus, in_specs=in_specs, out_specs=out_specs, check_vma=False
    )
```
